512 devices in a mesh: sp: 32 (over z, x), tp: 16 (over y, core).
Axes of the slice: x: 4, y: 8, z: 8, core: 2. Of those that a mesh axis runs over, the one named last changes fastest.
Arguments:
- outer_gate: bfloat16 [8192, 2048], P('sp', 'tp'), may hold values from -6 to 6
- inner_gate: bfloat16 [8192, 2048], P('sp', 'tp'), may hold values from -6 to 6
- conv_input: bfloat16 [8192, 2048], P('sp', 'tp'), may hold values from -6 to 6
- conv_weight: bfloat16 [3, 2048], P(None, 'tp'), may hold values from -3.5 to 3.5
- doc_ids: int32 [8192], P('sp'), may hold values from 0 to 15, as said below
- output_weight: bfloat16 [2048, 4096], P(None, 'tp'), may hold values from -0.125 to 0.125
- residual: bfloat16 [8192, 4096], P('sp', 'tp'), as said below
- norm_gain: bfloat16 [4096], P('tp'), may hold values from 0.099609375 to 1.8984375
- expert_ids: int32 [8192, 2], P('sp'), may hold values from 0 to 31, all different within a row; in each aligned block of 256 rows (0 to 255, 256 to 511, ...) at most 32 rows name the same one
- group_weight: float32 [8192], P('sp'), may hold values from 0.25 to 1
- expert_weight: float32 [8192, 2], P('sp'), may hold values from 0.05 to 1
- gate_weight: bfloat16 [32, 4096, 2048], P('sp', None, 'tp'), may hold values from -0.09375 to 0.09375
- up_weight: bfloat16 [32, 4096, 2048], P('sp', None, 'tp'), may hold values from -0.09375 to 0.09375
- down_weight: bfloat16 [32, 2048, 4096], P('sp', None, 'tp'), may hold values from -0.125 to 0.125
Outputs:
- layer_out: bfloat16 [8192, 4096], P('sp', 'tp')
The draws below stay inside these ranges and needn't reach their ends.
Inputs may be any that keep to these rules, and one draw needn't show every extreme that they name: `expert_ids`: within the 256 rows of one index of sp no expert is named more than 32 times, a bound that some block reaches; the two experts of a row differ. `doc_ids`: never falling along positions, rising by one at each document's start; every document has 256 to 768 positions, and one exactly 768. `residual`: Columns' scales are of order one to ten.
All inputs are finite; a program needn't handle non-finite values.
Results may differ from the reference program's by a relative error of at most 0.009.
Values may be sent and summed in bfloat16 or wider, within the bound.
A program may use at most 64 MiB of HBM per device.

```python
import math
import jax
import jax.numpy as jnp
import numpy as np
from jax import lax

D = 4096
BRANCH = 2048
FFN = 2048
TAPS = 3
TOK = 256
TOKENS = 8192
EXPERTS = 32
CAP = 32
N_SP = 32


def draw_residual(key, part):
    column_scale = 10.0 ** (jnp.arange(D, dtype=jnp.float32) / D)
    base = jax.random.normal(key, (TOKENS, D), jnp.float32)
    return (base * column_scale * 0.5).astype(jnp.bfloat16)


def draw_doc_ids(key, part):
    bound_total = N_SP // 2 - 1
    jitters = jax.random.randint(jax.random.fold_in(key, 11), (bound_total,), 0, TOK, dtype=jnp.int32)
    longest = jax.random.randint(jax.random.fold_in(key, 13), (), 0, bound_total, dtype=jnp.int32)
    marker = jnp.arange(bound_total, dtype=jnp.int32)
    jitters = jnp.where(marker == longest - 1, 0, jitters)
    jitters = jnp.where(marker == longest, TOK, jitters)
    starts = (marker + 1) * (2 * TOK) + jitters
    positions = jnp.arange(TOKENS, dtype=jnp.int32)
    return jnp.sum((positions[:, None] >= starts[None, :]).astype(jnp.int32), axis=1).astype(jnp.int32)


def level_of(rng, extent, pieces, least, largest):
    loudness, own = 1.0, jax.random.fold_in(rng, 6)
    for axis_at, blocks in pieces:
        heights = jnp.exp(jax.random.uniform(jax.random.fold_in(own, axis_at), (blocks,), jnp.float32, least / len(pieces), largest / len(pieces)))
        loudness = loudness * jnp.repeat(heights, extent[axis_at] // blocks).reshape([-1 if axis == axis_at else 1 for axis in range(len(extent))])
    return loudness


def deal_out(stream_key, own, number, rows, amount, top, bound, lean):
    sequence = jax.random.permutation(stream_key, amount)
    heavy_load, ordinary = shares(amount, rows * top, bound, lean, True), shares(amount, rows * top, bound, lean, False)
    places = jnp.arange(amount)

    def named(tallies, turn):
        used = int((tallies > 0).sum())
        fixed = max(1, used // 4)
        moved = fixed + (places - fixed + turn * (used - fixed)) % max(1, amount - fixed)
        return jnp.zeros((amount,), jnp.int32).at[sequence[jnp.where(places < fixed, places, moved)]].set(jnp.asarray(tallies, jnp.int32))

    tallies = jnp.where(number % 4 == 0, named(heavy_load, number // 4), named(ordinary, number - number // 4 - 1))
    mixed = jax.random.permutation(jax.random.fold_in(own, 3), amount)
    source_of, sink = mixed[0:amount // 2 * 2:2], mixed[1:amount // 2 * 2:2]
    margin = jnp.minimum(tallies[source_of] - 1, bound - tallies[sink]) // 2
    margin = jnp.where((source_of == sequence[0]) | (sink == sequence[0]) | (tallies[sink] == 0), 0, jnp.maximum(margin, 0))
    moved = jax.random.randint(jax.random.fold_in(own, 4), (amount // 2,), 0, 1 << 20) % (margin + 1)
    tallies = tallies.at[source_of].add(-moved).at[sink].add(moved)
    items = jnp.searchsorted(jnp.cumsum(tallies), jnp.arange(rows * top), side="right").astype(jnp.int32)
    grid = items.reshape(top, rows).T
    grid = grid[jax.random.permutation(jax.random.fold_in(own, 1), rows)]
    turn = jax.random.randint(jax.random.fold_in(own, 2), (rows, 1), 0, top)
    return jnp.take_along_axis(grid, (jnp.arange(top)[None, :] + turn) % top, axis=1)


def shares(count, total, reach, skew, full):
    portions = [(1 << 20) // math.isqrt(rank ** skew) + 1 for rank in range(1, count + 1)]
    largest = reach if full else min(reach, max(-(-total // count), total * portions[0] // sum(portions)))
    least = 1 if total - largest >= count - 1 else 0
    counts, rest = [largest] + [least] * (count - 1), total - largest - least * (count - 1)
    while rest > 0:
        candidates = [i for i in range(1, count) if counts[i] < largest] or [i for i in range(1, count) if counts[i] < reach]
        whole, remaining = sum([portions[i] for i in candidates]), rest
        for i in candidates:
            more = min(reach - counts[i], max(1, remaining * portions[i] // whole), rest)
            counts[i] = counts[i] + more
            rest = rest - more
    return np.array(counts)


def centred(rng, extent, width, limit, cuts=(), kind=jnp.bfloat16):
    values = jax.random.normal(rng, extent, jnp.float32) * width
    if len(cuts) > 0:
        values = level_of(rng, extent, cuts, -0.22, 0.18) * values
    return jnp.clip(values, min=-limit, max=limit).astype(kind)


def setup_inputs(seed: int = 0) -> dict:
    key_of = jax.random.split(jax.random.key(seed), 15)
    outer_gate = centred(key_of[0], (TOKENS, BRANCH), 1.0, 6.0, ((0, 32), (1, 16)))
    inner_gate = centred(key_of[1], (TOKENS, BRANCH), 1.0, 6.0, ((0, 32), (1, 16)))
    conv_input = centred(key_of[2], (TOKENS, BRANCH), 1.0, 6.0, ((0, 32), (1, 16)))
    conv_weight = centred(key_of[3], (TAPS, BRANCH), TAPS ** -0.5, 3.5, ((1, 16),))
    doc_ids = draw_doc_ids(jax.random.fold_in(key_of[14], 71), 0)
    output_weight = centred(key_of[5], (BRANCH, D), BRANCH ** -0.5, 0.125, ((1, 16),))
    residual = draw_residual(jax.random.fold_in(key_of[14], 71), 0)
    norm_gain = jnp.clip(1.0 + 0.18 * jax.random.normal(key_of[7], (D,), jnp.float32), 0.099609375, 1.8984375).astype(jnp.bfloat16)
    expert_ids_keys = jax.random.split(jax.random.fold_in(key_of[8], 1), TOKENS // TOK)
    expert_ids_turns = jax.random.permutation(jax.random.fold_in(key_of[8], 3), TOKENS // TOK)
    expert_ids = jax.vmap(lambda own, number: deal_out(jax.random.fold_in(key_of[8], 2), own, number, TOK, EXPERTS, 2, CAP, 2))(expert_ids_keys, expert_ids_turns).reshape((TOKENS, 2))
    group_weight = jnp.clip(0.25 + 0.75 * jax.random.uniform(key_of[9], (TOKENS,), jnp.float32) ** level_of(key_of[9], (TOKENS,), ((0, 32),), -0.2, 0.2), 0.25, 1.0)
    expert_weight = jnp.clip(jnp.exp(math.log(1.0) - 2.9957323 * jax.random.uniform(key_of[10], (TOKENS, 2), jnp.float32) ** level_of(key_of[10], (TOKENS, 2), ((0, 32),), -0.2, 0.2)), 0.05, 1.0)
    gate_weight = centred(key_of[11], (EXPERTS, D, FFN), D ** -0.5, 0.09375, ((0, 32), (2, 16)))
    up_weight = centred(key_of[12], (EXPERTS, D, FFN), D ** -0.5, 0.09375, ((0, 32), (2, 16)))
    down_weight = centred(key_of[13], (EXPERTS, FFN, D), FFN ** -0.5, 0.125, ((0, 32), (2, 16)))
    return {"outer_gate": outer_gate, "inner_gate": inner_gate, "conv_input": conv_input, "conv_weight": conv_weight, "doc_ids": doc_ids, "output_weight": output_weight, "residual": residual, "norm_gain": norm_gain, "expert_ids": expert_ids, "group_weight": group_weight, "expert_weight": expert_weight, "gate_weight": gate_weight, "up_weight": up_weight, "down_weight": down_weight}


EPS = 1e-06

def reference(outer_gate, inner_gate, conv_input, conv_weight, doc_ids, output_weight, residual, norm_gain, expert_ids, group_weight, expert_weight, gate_weight, up_weight, down_weight):
    products = inner_gate.astype(jnp.float32) * conv_input.astype(jnp.float32)
    taps = conv_weight.astype(jnp.float32)
    conv = taps[2] * products
    for shift_by in (1, 2):
        earlier = jnp.pad(products, ((shift_by, 0), (0, 0)))[:-shift_by]
        earlier_docs = jnp.pad(doc_ids, (shift_by, 0), constant_values=-1)[:-shift_by]
        same_doc = (earlier_docs == doc_ids)[:, None]
        conv = conv + jnp.where(same_doc, taps[2 - shift_by] * earlier, 0.0)
    branch = (outer_gate.astype(jnp.float32) * conv).astype(jnp.bfloat16)
    branch_sum = jnp.dot(branch, output_weight, preferred_element_type=jnp.float32)
    resid = (residual.astype(jnp.float32) + branch_sum).astype(jnp.bfloat16)
    resid_wide = resid.astype(jnp.float32)
    scale = lax.rsqrt(lax.optimization_barrier(jnp.mean(resid_wide * resid_wide, axis=1, keepdims=True)) + EPS)
    normed = (resid_wide * scale * norm_gain.astype(jnp.float32)).astype(jnp.bfloat16)
    mix_weight = group_weight[:, None] * expert_weight / lax.optimization_barrier(jnp.sum(expert_weight, axis=1, keepdims=True))
    flat_experts = expert_ids.reshape(N_SP, 2 * TOK)
    onehot = (flat_experts[:, :, None] == jnp.arange(EXPERTS, dtype=jnp.int32)[None, None, :]).astype(jnp.int32)
    slot_rank = lax.optimization_barrier(jnp.sum((jnp.cumsum(onehot, axis=1) - onehot) * onehot, axis=2)).astype(jnp.int32)
    slot_index = flat_experts * CAP + slot_rank
    token_of = jnp.broadcast_to(jnp.arange(2 * TOK, dtype=jnp.int32) // 2, slot_index.shape)
    group_index = jnp.arange(N_SP, dtype=jnp.int32)[:, None]
    token_table = jnp.full((N_SP, EXPERTS * CAP), TOK, jnp.int32).at[group_index, slot_index].set(token_of)
    token_table = token_table.reshape(N_SP, EXPERTS, CAP)
    grouped = jnp.concatenate([normed.reshape(N_SP, TOK, D), jnp.zeros((N_SP, 1, D), jnp.bfloat16)], axis=1)

    def one_expert(expert):
        chosen = lax.dynamic_index_in_dim(token_table, expert, 1, keepdims=False)
        routed = grouped[group_index, chosen].reshape(N_SP * CAP, D)
        gate_val = jnp.dot(routed, gate_weight[expert], preferred_element_type=jnp.float32)
        up_val = jnp.dot(routed, up_weight[expert], preferred_element_type=jnp.float32)
        hidden = (jax.nn.silu(gate_val) * up_val).astype(jnp.bfloat16)
        result = jnp.dot(hidden, down_weight[expert], preferred_element_type=jnp.float32).astype(jnp.bfloat16)
        return result.reshape(N_SP, CAP, D)
    expert_out = lax.map(one_expert, jnp.arange(EXPERTS, dtype=jnp.int32))
    picked = expert_out[flat_experts, group_index, slot_rank].reshape(TOKENS, 2, D).astype(jnp.float32)
    routed_sum = lax.optimization_barrier(jnp.sum(picked * mix_weight[:, :, None], axis=1))
    return (resid_wide + routed_sum).astype(jnp.bfloat16)
```

```python
import functools
import jax
import jax.numpy as jnp
from jax import lax
from jax.experimental import pallas as pl
from jax.experimental.pallas import tpu as pltpu
from jax.sharding import PartitionSpec as P

EPS = 1e-06
MESH = pl.DeviceIdType.MESH
F32 = jnp.float32
BF16 = jnp.bfloat16

SP, NX, NZ = 32, 4, 8
TP, NY = 16, 8
ROWS = 256
COLS = 256
CH = 128
CAP = 32
SLOTS = SP * CAP
PIECES = 4
PROWS = SLOTS // PIECES
BROWS = 288
BPIECES = 2
BPROWS = BROWS // BPIECES


def rdma(src, dst, ssem, rsem, dev):
    return pltpu.make_async_remote_copy(
        src_ref=src, dst_ref=dst, send_sem=ssem, recv_sem=rsem, device_id=dev, device_id_type=MESH
    )


class Ring:
    def __init__(self, buf, pieces, prows, rsem, dsem, ssem, s, y, c):
        self.buf, self.pieces, self.prows = buf, pieces, prows
        self.rsem, self.dsem, self.ssem = rsem, dsem, ssem
        self.s, self.y, self.c = s, y, c
        self.plus = (s, 2 * ((y + 1) % NY) + c)
        self.minus = (s, 2 * ((y + NY - 1) % NY) + c)
        self.partner = (s, 2 * y + (1 - c))

    def at(self, chunk, p):
        return self.buf.at[chunk, pl.ds(pl.multiple_of(p * self.prows, 16), self.prows)]

    def ring(self, origin, p, dev):
        ref = self.at(2 * origin + self.c, p)
        return rdma(ref, ref, self.ssem, self.rsem.at[origin, p], dev)

    def local(self, origin, core, p):
        ref = self.at(2 * origin + core, p)
        return rdma(ref, ref, self.ssem, self.dsem.at[origin, p], self.partner)

    def begin(self, p):
        self.ring(self.y, p, self.plus).start()
        self.ring(self.y, p, self.minus).start()
        self.local(self.y, self.c, p).start()

    def own(self, p, compute):
        compute(2 * self.y + self.c, p)

    def arrivals(self, k, p, compute):
        half = self.pieces // 2
        low, high = p < half, p >= half
        up = (self.y + NY - k) % NY
        down = (self.y + k) % NY
        c = self.c

        @pl.when((k < 4) | low)
        def _():
            self.ring(up, p, self.plus).wait_recv()

            @pl.when((k < 3) | ((k == 3) & low))
            def _():
                self.ring(up, p, self.plus).start()

            self.local(up, c, p).start()

        @pl.when((k < 4) | high)
        def _():
            self.ring(down, p, self.minus).wait_recv()

            @pl.when((k < 3) | ((k == 3) & high))
            def _():
                self.ring(down, p, self.minus).start()

            self.local(down, c, p).start()

        compute(2 * up + c, p)

        @pl.when(k < 4)
        def _():
            compute(2 * down + c, p)

        pup = (self.y + NY - (k - 1)) % NY
        pdown = (self.y + (k - 1)) % NY
        self.local(pup, 1 - c, p).wait_recv()
        compute(2 * pup + 1 - c, p)

        @pl.when(k > 1)
        def _():
            self.local(pdown, 1 - c, p).wait_recv()
            compute(2 * pdown + 1 - c, p)

    def steps(self, compute):
        n = self.pieces

        def body(j, carry):
            self.arrivals(1 + j // n, j % n, compute)
            return carry

        lax.fori_loop(0, 4 * n, body, 0)

    def last(self, p, compute):
        far = (self.y + 4) % NY
        self.local(far, 1 - self.c, p).wait_recv()
        compute(2 * far + 1 - self.c, p)

    def drain(self):
        ref = self.buf.at[0:15]
        pltpu.make_async_copy(ref, ref, self.ssem).wait()


def kernel(
    og, ig, ci, cw, docs, resin, gain, ids, gw, ew, wo_hbm, wg_hbm, wu_hbm, wd_hbm,
    out,
    wo, wgu, wd, wsem,
    ext_p, ext_d, halo_p, halo_d, hsem,
    bbuf, bacc, brs, bds, bss,
    resid, sel, pick0, pick1, mixw,
    send, esem, els,
    xbuf, xacc, ssum, xrs, xds, xss,
    hbuf, hacc, hrs, hds, hss,
    obuf, ret, osem, ols,
):
    s = lax.axis_index("sp")
    t = lax.axis_index("tp")
    y, c = t // 2, t % 2
    z, x = s // NX, s % NX
    nxt = (s + 1) % SP

    loads = [
        pltpu.make_async_copy(wo_hbm, wo, wsem.at[0]),
        pltpu.make_async_copy(wg_hbm, wgu.at[:, 0:CH], wsem.at[1]),
        pltpu.make_async_copy(wu_hbm, wgu.at[:, CH : 2 * CH], wsem.at[2]),
        pltpu.make_async_copy(wd_hbm, wd, wsem.at[3]),
    ]
    for load in loads:
        load.start()

    barrier = pltpu.get_barrier_semaphore()

    def greet(i, carry):
        pl.semaphore_signal(barrier, inc=1, device_id=((s + i) % SP, t), device_id_type=MESH)
        return carry

    lax.fori_loop(1, SP, greet, 0)
    for peer in (2 * ((y + 1) % NY) + c, 2 * ((y + NY - 1) % NY) + c, 2 * y + 1 - c):
        pl.semaphore_signal(barrier, inc=1, device_id=(s, peer), device_id_type=MESH)

    ext_p[8:264, :] = ig[...].astype(F32) * ci[...].astype(F32)
    id0, id1 = ids[0:1, :], ids[1:2, :]
    expert = lax.broadcasted_iota(jnp.int32, (SP, ROWS), 0)
    is0, is1 = expert == id0, expert == id1
    named = jnp.where(is0 | is1, 1.0, 0.0).astype(BF16)
    before = lax.broadcasted_iota(jnp.int32, (ROWS, ROWS), 0) < lax.broadcasted_iota(
        jnp.int32, (ROWS, ROWS), 1
    )
    ahead = jnp.dot(named, jnp.where(before, 1.0, 0.0).astype(BF16), preferred_element_type=F32)
    rank0 = jnp.sum(jnp.where(is0, ahead, 0.0), axis=0, keepdims=True)
    rank1 = jnp.sum(jnp.where(is1, ahead, 0.0), axis=0, keepdims=True)
    slot0 = id0.astype(F32) * CAP + rank0
    slot1 = id1.astype(F32) * CAP + rank1
    e0, e1 = ew[0:1, :], ew[1:2, :]
    esum = e0 + e1
    group = gw[...]
    table = jnp.concatenate(
        [
            docs[...].astype(F32),
            slot0,
            slot1,
            group * e0 / esum,
            group * e1 / esum,
            jnp.zeros((CH - 5, ROWS), F32),
        ],
        axis=0,
    )
    columns = table.T
    ext_d[8:264, :] = jnp.broadcast_to(columns[:, 0:1], (ROWS, CH))
    mixw[...] = columns

    pl.semaphore_wait(barrier, SP - 1 + 3)

    halos = [
        rdma(ext_p.at[256:264], halo_p, hsem.at[0], hsem.at[1], (nxt, t)),
        rdma(ext_d.at[256:264], halo_d, hsem.at[2], hsem.at[3], (nxt, t)),
    ]
    for halo in halos:
        halo.start()
    for halo in halos:
        halo.wait_recv()
    ext_p[0:8, :] = halo_p[...]
    ext_d[0:8, :] = halo_d[...]

    taps = cw[...].astype(F32)
    own_docs = ext_d[8:264, :]
    row = lax.broadcasted_iota(jnp.int32, (ROWS, CH), 0)
    conv = taps[2:3, :] * ext_p[8:264, :]
    for shift in (1, 2):
        same = (ext_d[8 - shift : 264 - shift, :] == own_docs) & ((row >= shift) | (s > 0))
        conv = conv + jnp.where(same, taps[2 - shift : 3 - shift, :] * ext_p[8 - shift : 264 - shift, :], 0.0)
    bbuf[t, 0:ROWS, :] = (og[...].astype(F32) * conv).astype(BF16)
    bbuf[t, ROWS:BROWS, :] = jnp.concatenate(
        [gain[...].astype(F32), jnp.zeros((BROWS - ROWS - 2, CH), F32)], axis=0
    ).astype(BF16)

    branch = Ring(bbuf, BPIECES, BPROWS, brs, bds, bss, s, y, c)
    for p in range(BPIECES):
        branch.begin(p)

    bacc[...] = jnp.zeros_like(bacc)
    loads[0].wait()

    def project(chunk, p):
        rows = pl.ds(pl.multiple_of(p * BPROWS, 16), BPROWS)
        weights = wo[pl.ds(pl.multiple_of(chunk * CH, CH), CH), :]
        bacc[rows, :] += jnp.dot(bbuf[chunk, rows, :], weights, preferred_element_type=F32)

    for p in range(BPIECES):
        branch.own(p, project)

    def tables(i, carry):
        rows = pl.ds(pl.multiple_of(i * 256, 256), 256)
        slot = (lax.broadcasted_iota(jnp.int32, (256, ROWS), 0) + i * 256).astype(F32)
        sel[rows, :] = jnp.where((slot == slot0) | (slot == slot1), 1.0, 0.0).astype(BF16)
        return carry

    lax.fori_loop(0, SLOTS // 256, tables, 0)

    branch.steps(project)
    for p in range(BPIECES):
        branch.last(p, project)

    resid[...] = (resin[...].astype(F32) + bacc[0:ROWS, :]).astype(BF16)

    def group_rows(i, carry):
        rows = pl.ds(pl.multiple_of(i * 256, 256), 256)
        send[rows, :] = jnp.dot(sel[rows, :], resid[...], preferred_element_type=F32).astype(BF16)
        return carry

    lax.fori_loop(0, SLOTS // 256, group_rows, 0)

    def place(p, d_z, d_x):
        return p * 8 + (d_z // 2) * 2 + d_x // 2

    def partners(p):
        px, pz = p // 2, p % 2
        for zh in (2, 1, 3, 0):
            for xh in (1, 0):
                yield (px, pz, zh, xh), (z + pz + 2 * zh) % NZ, (x + px + 2 * xh) % NX

    def block(ref, i):
        return ref.at[pl.ds(pl.multiple_of(i * CAP, CAP), CAP)]

    for p in range(PIECES):
        mine = place(p, z, x)
        for which, dz, dx in partners(p):
            d = dz * NX + dx
            dst = block(xbuf.at[t], mine)
            if which == (0, 0, 0, 0):
                pltpu.make_async_copy(block(send, d), dst, els.at[0]).start()
            else:
                rdma(block(send, d), dst, esem.at[SP], esem.at[mine], (d, t)).start()

    xacc[...] = jnp.zeros_like(xacc)
    ssum[...] = jnp.zeros_like(ssum)
    hacc[...] = jnp.zeros_like(hacc)
    for load in loads[1:3]:
        load.wait()

    def prows(p):
        return pl.ds(pl.multiple_of(p * PROWS, PROWS), PROWS)

    def widen(chunk, p):
        rows = prows(p)
        gains = bbuf[chunk, pl.ds(ROWS, 16), :].astype(F32)
        part = xbuf[chunk, rows, :].astype(F32)
        left, right = part[:, :CH], part[:, CH:]
        ssum[rows, :] += left * left + right * right
        scaled = jnp.concatenate([left * gains[0:1, :], right * gains[1:2, :]], axis=1).astype(BF16)
        weights = wgu[pl.ds(pl.multiple_of(chunk * COLS, COLS), COLS), :]
        xacc[rows, :] += jnp.dot(scaled, weights, preferred_element_type=F32)

    wide = Ring(xbuf, PIECES, PROWS, xrs, xds, xss, s, y, c)
    for p in range(PIECES):
        for which, dz, dx in partners(p):
            src = place(p, dz, dx)
            dst = block(xbuf.at[t], src)
            if which == (0, 0, 0, 0):
                pltpu.make_async_copy(dst, dst, els.at[0]).wait()
            else:
                rdma(dst, dst, esem.at[SP], esem.at[src], (s, t)).wait_recv()
        wide.begin(p)

    def own_rows(p, carry):
        wide.own(p, widen)
        return carry

    lax.fori_loop(0, PIECES, own_rows, 0)

    slot_lane = lax.broadcasted_iota(jnp.int32, (ROWS, SLOTS), 1).astype(F32)
    pick0[...] = jnp.where(slot_lane == mixw[:, 1:2], 1.0, 0.0).astype(BF16)
    pick1[...] = jnp.where(slot_lane == mixw[:, 2:3], 1.0, 0.0).astype(BF16)

    wide.steps(widen)

    deep = Ring(hbuf, PIECES, PROWS, hrs, hds, hss, s, y, c)

    def finish(p, carry):
        wide.last(p, widen)
        rows = prows(p)
        mean = jnp.sum(ssum[rows, :], axis=1, keepdims=True) / (TP * COLS)
        scale = lax.rsqrt(mean + EPS)
        gate = xacc[rows, 0:CH] * scale
        up = xacc[rows, CH : 2 * CH] * scale
        hbuf[t, rows, :] = (gate * jax.nn.sigmoid(gate) * up).astype(BF16)
        deep.begin(p)
        return carry

    lax.fori_loop(0, PIECES, finish, 0)
    loads[3].wait()

    def lower(chunk, p):
        rows = prows(p)
        weights = wd[pl.ds(pl.multiple_of(chunk * CH, CH), CH), :]
        hacc[rows, :] += jnp.dot(hbuf[chunk, rows, :], weights, preferred_element_type=F32)

    def own_hidden(p, carry):
        deep.own(p, lower)
        return carry

    lax.fori_loop(0, PIECES, own_hidden, 0)
    deep.steps(lower)

    for p in range(PIECES):
        deep.last(p, lower)
        rows = slice(p * PROWS, (p + 1) * PROWS)
        obuf[rows, :] = hacc[rows, :].astype(BF16)
        for which, dz, dx in partners(p):
            d = dz * NX + dx
            src = block(obuf, place(p, dz, dx))
            if which == (0, 0, 0, 0):
                pltpu.make_async_copy(src, block(ret, s), ols.at[0]).start()
            else:
                rdma(src, block(ret, s), osem.at[SP], osem.at[s], (d, t)).start()

    def arrive(i, carry):
        d = (s + i) % SP
        rdma(block(ret, d), block(ret, d), osem.at[SP], osem.at[d], (s, t)).wait_recv()
        return carry

    pltpu.make_async_copy(block(ret, s), block(ret, s), ols.at[0]).wait()
    lax.fori_loop(1, SP, arrive, 0)

    got0 = jnp.dot(pick0[...], ret[...], preferred_element_type=F32)
    got1 = jnp.dot(pick1[...], ret[...], preferred_element_type=F32)
    routed = got0 * mixw[:, 3:4] + got1 * mixw[:, 4:5]
    out[...] = (resid[...].astype(F32) + routed).astype(BF16)

    for halo in halos:
        halo.wait_send()
    branch.drain()
    rest = send.at[0 : SLOTS - CAP]
    pltpu.make_async_copy(rest, rest, esem.at[SP]).wait()
    wide.drain()
    deep.drain()
    rest = obuf.at[0 : SLOTS - CAP]
    pltpu.make_async_copy(rest, rest, osem.at[SP]).wait()


def per_device(
    outer_gate, inner_gate, conv_input, conv_weight, doc_ids, output_weight, residual,
    norm_gain, expert_ids, group_weight, expert_weight, gate_weight, up_weight, down_weight,
):
    dma = pltpu.SemaphoreType.DMA
    vmem = pl.BlockSpec(memory_space=pltpu.VMEM)
    hbm = pl.BlockSpec(memory_space=pl.ANY)
    scratch = [
        pltpu.VMEM((TP * CH, COLS), BF16),
        pltpu.VMEM((TP * COLS, 2 * CH), BF16),
        pltpu.VMEM((TP * CH, COLS), BF16),
        dma((4,)),
        pltpu.VMEM((264, CH), F32),
        pltpu.VMEM((264, CH), F32),
        pltpu.VMEM((8, CH), F32),
        pltpu.VMEM((8, CH), F32),
        dma((4,)),
        pltpu.VMEM((TP, BROWS, CH), BF16),
        pltpu.VMEM((BROWS, COLS), F32),
        dma((NY, BPIECES)),
        dma((NY, BPIECES)),
        dma,
        pltpu.VMEM((ROWS, COLS), BF16),
        pltpu.VMEM((SLOTS, ROWS), BF16),
        pltpu.VMEM((ROWS, SLOTS), BF16),
        pltpu.VMEM((ROWS, SLOTS), BF16),
        pltpu.VMEM((ROWS, CH), F32),
        pltpu.VMEM((SLOTS, COLS), BF16),
        dma((SP + 1,)),
        dma((1,)),
        pltpu.VMEM((TP, SLOTS, COLS), BF16),
        pltpu.VMEM((SLOTS, 2 * CH), F32),
        pltpu.VMEM((SLOTS, CH), F32),
        dma((NY, PIECES)),
        dma((NY, PIECES)),
        dma,
        pltpu.VMEM((TP, SLOTS, CH), BF16),
        pltpu.VMEM((SLOTS, COLS), F32),
        dma((NY, PIECES)),
        dma((NY, PIECES)),
        dma,
        pltpu.VMEM((SLOTS, COLS), BF16),
        pltpu.VMEM((SLOTS, COLS), BF16),
        dma((SP + 1,)),
        dma((1,)),
    ]
    return pl.pallas_call(
        kernel,
        name="layer",
        out_shape=jax.ShapeDtypeStruct((ROWS, COLS), BF16),
        in_specs=[vmem] * 10 + [hbm] * 4,
        out_specs=vmem,
        scratch_shapes=scratch,
        compiler_params=pltpu.CompilerParams(
            collective_id=0, has_side_effects=True, vmem_limit_bytes=56 * 1024 * 1024
        ),
    )(
        outer_gate,
        inner_gate,
        conv_input,
        conv_weight,
        doc_ids.reshape(1, ROWS),
        residual,
        norm_gain.reshape(2, CH),
        expert_ids.T,
        group_weight.reshape(1, ROWS),
        expert_weight.T,
        output_weight,
        gate_weight[0],
        up_weight[0],
        down_weight[0],
    )


def solution(mesh):
    return jax.shard_map(
        per_device,
        mesh=mesh,
        in_specs=(
            P("sp", "tp"),
            P("sp", "tp"),
            P("sp", "tp"),
            P(None, "tp"),
            P("sp"),
            P(None, "tp"),
            P("sp", "tp"),
            P("tp"),
            P("sp", None),
            P("sp"),
            P("sp", None),
            P("sp", None, "tp"),
            P("sp", None, "tp"),
            P("sp", None, "tp"),
        ),
        out_specs=P("sp", "tp"),
        check_vma=False,
    )
```

```python
import functools
import jax
import jax.numpy as jnp
from jax import lax
from jax.experimental import pallas as pl
from jax.experimental.pallas import tpu as pltpu
from jax.sharding import PartitionSpec as P

EPS = 1e-06
MESH = pl.DeviceIdType.MESH
F32 = jnp.float32
BF16 = jnp.bfloat16

SP, NX, NZ = 32, 4, 8
TP, NY = 16, 8
ROWS = 256
COLS = 256
CH = 128
CAP = 32
SLOTS = SP * CAP
PIECES = 4
PROWS = SLOTS // PIECES
PER = SP // PIECES
DELAY = (1, 1)
ZORDER = (0, 1, 6, 3, 5, 4, 7, 2)
BROWS = 272
BSPLIT = ((0, 128), (128, 128), (256, 16))


def rdma(src, dst, ssem, rsem, dev):
    return pltpu.make_async_remote_copy(
        src_ref=src, dst_ref=dst, send_sem=ssem, recv_sem=rsem, device_id=dev, device_id_type=MESH
    )


class Ring:
    def __init__(self, buf, pieces, prows, rsem, dsem, ssem, s, y, c):
        self.buf, self.pieces, self.prows = buf, pieces, prows
        self.rsem, self.dsem, self.ssem = rsem, dsem, ssem
        self.s, self.y, self.c = s, y, c
        self.plus = (s, 2 * ((y + 1) % NY) + c)
        self.minus = (s, 2 * ((y + NY - 1) % NY) + c)
        self.partner = (s, 2 * y + (1 - c))

    def at(self, chunk, p):
        return self.buf.at[chunk, pl.ds(pl.multiple_of(p * self.prows, 16), self.prows)]

    def ring(self, origin, p, dev):
        ref = self.at(2 * origin + self.c, p)
        return rdma(ref, ref, self.ssem, self.rsem.at[origin, p], dev)

    def local(self, origin, core, p):
        ref = self.at(2 * origin + core, p)
        return rdma(ref, ref, self.ssem, self.dsem.at[origin, p], self.partner)

    def begin(self, p):
        self.ring(self.y, p, self.plus).start()
        self.ring(self.y, p, self.minus).start()
        self.local(self.y, self.c, p).start()

    def own(self, p, compute):
        compute(2 * self.y + self.c, p)

    def arrivals(self, k, p, compute):
        low, high = p % 2 == 0, p % 2 == 1
        up = (self.y + NY - k) % NY
        down = (self.y + k) % NY
        c = self.c

        @pl.when((k < 4) | low)
        def _():
            self.ring(up, p, self.plus).wait_recv()

            @pl.when((k < 3) | ((k == 3) & low))
            def _():
                self.ring(up, p, self.plus).start()

            self.local(up, c, p).start()

        @pl.when((k < 4) | high)
        def _():
            self.ring(down, p, self.minus).wait_recv()

            @pl.when((k < 3) | ((k == 3) & high))
            def _():
                self.ring(down, p, self.minus).start()

            self.local(down, c, p).start()

        compute(2 * up + c, p)

        @pl.when(k < 4)
        def _():
            compute(2 * down + c, p)

        pup = (self.y + NY - (k - 1)) % NY
        pdown = (self.y + (k - 1)) % NY
        self.local(pup, 1 - c, p).wait_recv()
        compute(2 * pup + 1 - c, p)

        @pl.when(k > 1)
        def _():
            self.local(pdown, 1 - c, p).wait_recv()
            compute(2 * pdown + 1 - c, p)

    def last(self, p, compute):
        far = (self.y + 4) % NY
        self.local(far, 1 - self.c, p).wait_recv()
        compute(2 * far + 1 - self.c, p)

    def drain(self):
        ref = self.buf.at[0:15]
        pltpu.make_async_copy(ref, ref, self.ssem).wait()


def kernel(
    og, ig, ci, cw, docs, resin, gain, ids, gw, ew, wo_hbm, wg_hbm, wu_hbm, wd_hbm,
    out,
    wo, wgu, wd, wsem,
    ext_p, ext_d, halo_p, halo_d, hsem,
    bbuf, bacc, brs, bds, bss,
    resid, sel, pick0, pick1, mixw,
    send, esem,
    xbuf, xacc, ssum, xrs, xds, xss,
    hbuf, hacc, hrs, hds, hss,
    obuf, ret, osem,
):
    s = lax.axis_index("sp")
    t = lax.axis_index("tp")
    y, c = t // 2, t % 2
    z, x = s // NX, s % NX
    nxt = (s + 1) % SP

    loads = [
        pltpu.make_async_copy(wo_hbm, wo, wsem.at[0]),
        pltpu.make_async_copy(wg_hbm, wgu.at[:, 0:CH], wsem.at[1]),
        pltpu.make_async_copy(wu_hbm, wgu.at[:, CH : 2 * CH], wsem.at[2]),
        pltpu.make_async_copy(wd_hbm, wd, wsem.at[3]),
    ]
    for load in loads:
        load.start()

    barrier = pltpu.get_barrier_semaphore()

    def greet(i, carry):
        pl.semaphore_signal(barrier, inc=1, device_id=((s + i) % SP, t), device_id_type=MESH)
        return carry

    lax.fori_loop(1, SP, greet, 0)
    for off in (1, 2, NY - 1, NY - 2):
        peer = 2 * ((y + off) % NY) + c
        pl.semaphore_signal(barrier, inc=1, device_id=(s, peer), device_id_type=MESH)
    pl.semaphore_signal(barrier, inc=1, device_id=(s, 2 * y + 1 - c), device_id_type=MESH)

    ext_p[8:264, :] = ig[...].astype(F32) * ci[...].astype(F32)
    id0, id1 = ids[0:1, :], ids[1:2, :]
    expert = lax.broadcasted_iota(jnp.int32, (SP, ROWS), 0)
    is0, is1 = expert == id0, expert == id1
    named = jnp.where(is0 | is1, 1.0, 0.0).astype(BF16)
    before = lax.broadcasted_iota(jnp.int32, (ROWS, ROWS), 0) < lax.broadcasted_iota(
        jnp.int32, (ROWS, ROWS), 1
    )
    ahead = jnp.dot(named, jnp.where(before, 1.0, 0.0).astype(BF16), preferred_element_type=F32)
    rank0 = jnp.sum(jnp.where(is0, ahead, 0.0), axis=0, keepdims=True)
    rank1 = jnp.sum(jnp.where(is1, ahead, 0.0), axis=0, keepdims=True)
    slot0 = id0.astype(F32) * CAP + rank0
    slot1 = id1.astype(F32) * CAP + rank1
    e0, e1 = ew[0:1, :], ew[1:2, :]
    esum = e0 + e1
    group = gw[...]
    table = jnp.concatenate(
        [
            docs[...].astype(F32),
            slot0,
            slot1,
            group * e0 / esum,
            group * e1 / esum,
            jnp.zeros((CH - 5, ROWS), F32),
        ],
        axis=0,
    )
    columns = table.T
    ext_d[8:264, :] = jnp.broadcast_to(columns[:, 0:1], (ROWS, CH))
    mixw[...] = columns

    taps = cw[...].astype(F32)

    def branch_rows(lo, hi):
        own_docs = ext_d[8 + lo : 8 + hi, :]
        row = lax.broadcasted_iota(jnp.int32, (hi - lo, CH), 0) + lo
        conv = taps[2:3, :] * ext_p[8 + lo : 8 + hi, :]
        for shift in (1, 2):
            rows = slice(8 + lo - shift, 8 + hi - shift)
            same = (ext_d[rows, :] == own_docs) & ((row >= shift) | (s > 0))
            conv = conv + jnp.where(same, taps[2 - shift : 3 - shift, :] * ext_p[rows, :], 0.0)
        return (og[lo:hi, :].astype(F32) * conv).astype(BF16)

    bbuf[t, 0:128, :] = branch_rows(128, 256)
    bbuf[t, 128:240, :] = branch_rows(16, 128)
    bbuf[t, 240:256, :] = jnp.concatenate(
        [gain[...].astype(F32), jnp.zeros((14, CH), F32)], axis=0
    ).astype(BF16)
    bacc[...] = jnp.zeros_like(bacc)

    pl.semaphore_wait(barrier, SP - 1 + 5)

    halos = [
        rdma(ext_p.at[256:264], halo_p, hsem.at[0], hsem.at[1], (nxt, t)),
        rdma(ext_d.at[256:264], halo_d, hsem.at[2], hsem.at[3], (nxt, t)),
    ]
    for halo in halos:
        halo.start()

    def near(off):
        return (y + off + NY) % NY

    def hop(origin, p, off):
        lo, size = BSPLIT[p]
        ref = bbuf.at[2 * origin + c, pl.ds(lo, size)]
        return rdma(ref, ref, bss, brs.at[origin, p], (s, 2 * near(off) + c))

    def across(origin, core, p):
        lo, size = BSPLIT[p]
        ref = bbuf.at[2 * origin + core, pl.ds(lo, size)]
        return rdma(ref, ref, bss, bds.at[origin, p], (s, 2 * y + 1 - c))

    def open_piece(p):
        for off in (2, -2, 1, -1):
            hop(y, p, off).start()
        across(y, c, p).start()

    open_piece(0)
    open_piece(1)
    for halo in halos:
        halo.wait_recv()
    ext_p[0:8, :] = halo_p[...]
    ext_d[0:8, :] = halo_d[...]
    bbuf[t, 256:272, :] = branch_rows(0, 16)
    open_piece(2)

    def far_side(p):
        return 1 if p != 1 else -1

    for p in range(3):
        for side in (1, -1):
            origin = near(-2 * side)
            hop(origin, p, side).wait_recv()
            if far_side(p) == side:
                hop(origin, p, 2 * side).start()
            hop(origin, p, side).start()
            across(origin, c, p).start()
        for side in (1, -1):
            origin = near(-side)
            hop(origin, p, side).wait_recv()
            across(origin, c, p).start()

    loads[0].wait()

    def project(first, count, core):
        def one(i, carry):
            chunk = 2 * ((y + first + i) % NY) + core
            weights = wo[pl.ds(pl.multiple_of(chunk * CH, CH), CH), :]
            bacc[...] += jnp.dot(bbuf[chunk], weights, preferred_element_type=F32)
            return carry

        lax.fori_loop(0, count, one, 0)

    project(6, 5, c)

    def tables(i, carry):
        rows = pl.ds(pl.multiple_of(i * 256, 256), 256)
        slot = (lax.broadcasted_iota(jnp.int32, (256, ROWS), 0) + i * 256).astype(F32)
        sel[rows, :] = jnp.where((slot == slot0) | (slot == slot1), 1.0, 0.0).astype(BF16)
        return carry

    lax.fori_loop(0, SLOTS // 256, tables, 0)

    for off in (3, -3, 4):
        origin = near(off)
        for p in range(3):
            hop(origin, p, 1).wait_recv()
            across(origin, c, p).start()
    for off in (0, 1, -1, 2, -2):
        for p in range(3):
            across(near(off), 1 - c, p).wait_recv()
    project(6, 5, 1 - c)
    project(3, 3, c)
    for off in (3, -3, 4):
        for p in range(3):
            across(near(off), 1 - c, p).wait_recv()
    project(3, 3, 1 - c)

    for (lo, size), first in zip(((0, 128), (128, 112), (256, 16)), (128, 16, 0)):
        rows = slice(first, first + size)
        resid[rows, :] = (resin[rows, :].astype(F32) + bacc[lo : lo + size, :]).astype(BF16)

    def group_rows(i, carry):
        rows = pl.ds(pl.multiple_of(i * 256, 256), 256)
        send[rows, :] = jnp.dot(sel[rows, :], resid[...], preferred_element_type=F32).astype(BF16)
        return carry

    lax.fori_loop(0, SLOTS // 256, group_rows, 0)

    def block(ref, i):
        return ref.at[pl.ds(pl.multiple_of(i * CAP, CAP), CAP)]

    def offsets(q):
        return ZORDER[q // NX], q % NX

    for q in range(SP):
        dz, dx = offsets(q)
        d = ((z + dz) % NZ) * NX + (x + dx) % NX
        if q == 0:
            pltpu.make_async_copy(block(send, d), block(xbuf.at[t], q), esem.at[q]).start()
        else:
            rdma(block(send, d), block(xbuf.at[t], q), esem.at[SP], esem.at[q], (d, t)).start()

    xacc[...] = jnp.zeros_like(xacc)
    ssum[...] = jnp.zeros_like(ssum)
    hacc[...] = jnp.zeros_like(hacc)
    for load in loads[1:]:
        load.wait()

    def prows(p):
        return pl.ds(pl.multiple_of(p * PROWS, PROWS), PROWS)

    def widen(chunk, p):
        rows = prows(p)
        gains = bbuf[chunk, pl.ds(240, 16), :].astype(F32)
        part = xbuf[chunk, rows, :].astype(F32)
        left, right = part[:, :CH], part[:, CH:]
        ssum[rows, :] += left * left + right * right
        scaled = jnp.concatenate([left * gains[0:1, :], right * gains[1:2, :]], axis=1).astype(BF16)
        weights = wgu[pl.ds(pl.multiple_of(chunk * COLS, COLS), COLS), :]
        xacc[rows, :] += jnp.dot(scaled, weights, preferred_element_type=F32)

    def lower(chunk, p):
        rows = prows(p)
        weights = wd[pl.ds(pl.multiple_of(chunk * CH, CH), CH), :]
        hacc[rows, :] += jnp.dot(hbuf[chunk, rows, :], weights, preferred_element_type=F32)

    slot_lane = lax.broadcasted_iota(jnp.int32, (ROWS, SLOTS), 1).astype(F32)
    pick0[...] = jnp.where(slot_lane == mixw[:, 1:2], 1.0, 0.0).astype(BF16)
    pick1[...] = jnp.where(slot_lane == mixw[:, 2:3], 1.0, 0.0).astype(BF16)

    wide = Ring(xbuf, PIECES, PROWS, xrs, xds, xss, s, y, c)
    deep = Ring(hbuf, PIECES, PROWS, hrs, hds, hss, s, y, c)

    def enter(p):
        def one(i, carry):
            q = p * PER + i
            dst = block(xbuf.at[t], q)
            pltpu.make_async_copy(dst, dst, esem.at[q]).wait()
            return carry

        lax.fori_loop(0, PER, one, 0)
        wide.begin(p)
        wide.own(p, widen)

    def activate(p):
        wide.last(p, widen)
        rows = prows(p)
        mean = jnp.sum(ssum[rows, :], axis=1, keepdims=True) / (TP * COLS)
        scale = lax.rsqrt(mean + EPS)
        gate = xacc[rows, 0:CH] * scale
        up = xacc[rows, CH : 2 * CH] * scale
        hbuf[t, rows, :] = (gate * jax.nn.sigmoid(gate) * up).astype(BF16)
        deep.begin(p)
        deep.own(p, lower)

    def leave(p):
        deep.last(p, lower)
        rows = slice(p * PROWS, (p + 1) * PROWS)
        obuf[rows, :] = hacc[rows, :].astype(BF16)
        for q in range(p * PER, (p + 1) * PER):
            dz, dx = offsets(q)
            d = ((z + NZ - dz) % NZ) * NX + (x + NX - dx) % NX
            if q == 0:
                pltpu.make_async_copy(block(obuf, q), block(ret, s), osem.at[s]).start()
            else:
                rdma(block(obuf, q), block(ret, s), osem.at[SP], osem.at[s], (d, t)).start()

    def wave(j, carry):
        p = j % PIECES
        stage = j // PIECES - p * DELAY[0] // DELAY[1]

        @pl.when(stage == 0)
        def _():
            enter(p)

        @pl.when((stage >= 1) & (stage <= 4))
        def _():
            wide.arrivals(stage, p, widen)

        @pl.when(stage == 5)
        def _():
            activate(p)

        @pl.when((stage >= 6) & (stage <= 9))
        def _():
            deep.arrivals(stage - 5, p, lower)

        for piece in range(PIECES):

            @pl.when((stage == 10) & (p == piece))
            def _(piece=piece):
                leave(piece)

        return carry

    lax.fori_loop(0, PIECES * (11 + (PIECES - 1) * DELAY[0] // DELAY[1]), wave, 0)

    def arrive(d, carry):
        pltpu.make_async_copy(block(ret, d), block(ret, d), osem.at[d]).wait()
        return carry

    lax.fori_loop(0, SP, arrive, 0)

    got0 = jnp.dot(pick0[...], ret[...], preferred_element_type=F32)
    got1 = jnp.dot(pick1[...], ret[...], preferred_element_type=F32)
    routed = got0 * mixw[:, 3:4] + got1 * mixw[:, 4:5]
    out[...] = resid[...].astype(F32) + routed

    for halo in halos:
        halo.wait_send()
    rest = bbuf.at[0:15]
    pltpu.make_async_copy(rest, rest, bss).wait()
    rest = send.at[0 : SLOTS - CAP]
    pltpu.make_async_copy(rest, rest, esem.at[SP]).wait()
    wide.drain()
    deep.drain()
    rest = obuf.at[0 : SLOTS - CAP]
    pltpu.make_async_copy(rest, rest, osem.at[SP]).wait()


def per_device(
    outer_gate, inner_gate, conv_input, conv_weight, doc_ids, output_weight, residual,
    norm_gain, expert_ids, group_weight, expert_weight, gate_weight, up_weight, down_weight,
):
    dma = pltpu.SemaphoreType.DMA
    vmem = pl.BlockSpec(memory_space=pltpu.VMEM)
    hbm = pl.BlockSpec(memory_space=pl.ANY)
    scratch = [
        pltpu.VMEM((TP * CH, COLS), BF16),
        pltpu.VMEM((TP * COLS, 2 * CH), BF16),
        pltpu.VMEM((TP * CH, COLS), BF16),
        dma((4,)),
        pltpu.VMEM((264, CH), F32),
        pltpu.VMEM((264, CH), F32),
        pltpu.VMEM((8, CH), F32),
        pltpu.VMEM((8, CH), F32),
        dma((4,)),
        pltpu.VMEM((TP, BROWS, CH), BF16),
        pltpu.VMEM((BROWS, COLS), F32),
        dma((NY, 3)),
        dma((NY, 3)),
        dma,
        pltpu.VMEM((ROWS, COLS), BF16),
        pltpu.VMEM((SLOTS, ROWS), BF16),
        pltpu.VMEM((ROWS, SLOTS), BF16),
        pltpu.VMEM((ROWS, SLOTS), BF16),
        pltpu.VMEM((ROWS, CH), F32),
        pltpu.VMEM((SLOTS, COLS), BF16),
        dma((SP + 1,)),
        pltpu.VMEM((TP, SLOTS, COLS), BF16),
        pltpu.VMEM((SLOTS, 2 * CH), F32),
        pltpu.VMEM((SLOTS, CH), F32),
        dma((NY, PIECES)),
        dma((NY, PIECES)),
        dma,
        pltpu.VMEM((TP, SLOTS, CH), BF16),
        pltpu.VMEM((SLOTS, COLS), F32),
        dma((NY, PIECES)),
        dma((NY, PIECES)),
        dma,
        pltpu.VMEM((SLOTS, COLS), BF16),
        pltpu.VMEM((SLOTS, COLS), BF16),
        dma((SP + 1,)),
    ]
    return pl.pallas_call(
        kernel,
        name="layer",
        out_shape=jax.ShapeDtypeStruct((ROWS, COLS), F32),
        in_specs=[vmem] * 10 + [hbm] * 4,
        out_specs=vmem,
        scratch_shapes=scratch,
        compiler_params=pltpu.CompilerParams(
            collective_id=0, has_side_effects=True, vmem_limit_bytes=56 * 1024 * 1024
        ),
    )(
        outer_gate,
        inner_gate,
        conv_input,
        conv_weight,
        doc_ids.reshape(1, ROWS),
        residual,
        norm_gain.reshape(2, CH),
        expert_ids.T,
        group_weight.reshape(1, ROWS),
        expert_weight.T,
        output_weight,
        gate_weight[0],
        up_weight[0],
        down_weight[0],
    ).astype(BF16)


def solution(mesh):
    return jax.shard_map(
        per_device,
        mesh=mesh,
        in_specs=(
            P("sp", "tp"),
            P("sp", "tp"),
            P("sp", "tp"),
            P(None, "tp"),
            P("sp"),
            P(None, "tp"),
            P("sp", "tp"),
            P("tp"),
            P("sp", None),
            P("sp"),
            P("sp", None),
            P("sp", None, "tp"),
            P("sp", None, "tp"),
            P("sp", None, "tp"),
        ),
        out_specs=P("sp", "tp"),
        check_vma=False,
    )
```

```python
import functools
import jax
import jax.numpy as jnp
from jax import lax
from jax.experimental import pallas as pl
from jax.experimental.pallas import tpu as pltpu
from jax.sharding import PartitionSpec as P

EPS = 1e-06
MESH = pl.DeviceIdType.MESH
F32 = jnp.float32
BF16 = jnp.bfloat16

SP, NX, NZ = 32, 4, 8
TP, NY = 16, 8
ROWS = 256
COLS = 256
CH = 128
CAP = 32
SLOTS = SP * CAP
PIECES = 4
PROWS = SLOTS // PIECES
PER = SP // PIECES
DELAY = (1, 1)
ZORDER = (0, 1, 6, 3, 5, 4, 7, 2)
BROWS = 272
BSPLIT = ((0, 128), (128, 128), (256, 16))


def rdma(src, dst, ssem, rsem, dev):
    return pltpu.make_async_remote_copy(
        src_ref=src, dst_ref=dst, send_sem=ssem, recv_sem=rsem, device_id=dev, device_id_type=MESH
    )


class Ring:
    def __init__(self, buf, pieces, prows, rsem, dsem, fsem, ssem, s, y, c):
        self.buf, self.pieces, self.prows = buf, pieces, prows
        self.rsem, self.dsem, self.fsem, self.ssem = rsem, dsem, fsem, ssem
        self.s, self.y, self.c = s, y, c
        self.plus = (s, 2 * ((y + 1) % NY) + c)
        self.minus = (s, 2 * ((y + NY - 1) % NY) + c)
        self.partner = (s, 2 * y + (1 - c))

    def at(self, chunk, p):
        return self.buf.at[chunk, pl.ds(pl.multiple_of(p * self.prows, 16), self.prows)]

    def ring(self, origin, p, dev):
        ref = self.at(2 * origin + self.c, p)
        return rdma(ref, ref, self.ssem, self.rsem.at[origin, p], dev)

    def local(self, origin, core, p):
        ref = self.at(2 * origin + core, p)
        return rdma(ref, ref, self.ssem, self.dsem.at[origin, p], self.partner)

    def begin(self, p):
        self.ring(self.y, p, self.plus).start()
        self.ring(self.y, p, self.minus).start()
        self.local(self.y, self.c, p).start()

    def own(self, p, compute):
        compute(2 * self.y + self.c, p)

    def half(self, p, h, dev):
        rows = self.prows // 2
        far = self.buf.at[
            2 * h[0] + self.c, pl.ds(pl.multiple_of(p * self.prows + h[1] * rows, 16), rows)
        ]
        return rdma(far, far, self.ssem, self.fsem.at[h[1], p], dev)

    def arrivals(self, k, p, compute):
        up = (self.y + NY - k) % NY
        down = (self.y + k) % NY
        c = self.c

        @pl.when(k < 4)
        def _():
            for origin, side, h in ((up, self.plus, 0), (down, self.minus, 1)):
                self.ring(origin, p, side).wait_recv()

                @pl.when(k < 3)
                def _():
                    self.ring(origin, p, side).start()

                @pl.when(k == 3)
                def _():
                    self.half(p, (origin, h), side).start()

                self.local(origin, c, p).start()

        @pl.when(k == 4)
        def _():
            for h in (0, 1):
                self.half(p, (up, h), self.plus).wait_recv()
            self.local(up, c, p).start()

        compute(2 * up + c, p)

        @pl.when(k < 4)
        def _():
            compute(2 * down + c, p)

        pup = (self.y + NY - (k - 1)) % NY
        pdown = (self.y + (k - 1)) % NY
        self.local(pup, 1 - c, p).wait_recv()
        compute(2 * pup + 1 - c, p)

        @pl.when(k > 1)
        def _():
            self.local(pdown, 1 - c, p).wait_recv()
            compute(2 * pdown + 1 - c, p)

    def last(self, p, compute):
        far = (self.y + 4) % NY
        self.local(far, 1 - self.c, p).wait_recv()
        compute(2 * far + 1 - self.c, p)

    def drain(self):
        ref = self.buf.at[0:15]
        pltpu.make_async_copy(ref, ref, self.ssem).wait()


def kernel(
    og, ig, ci, cw, docs, resin, gain, ids, gw, ew, wo_hbm, wg_hbm, wu_hbm, wd_hbm,
    out,
    wo, wgu, wd, wsem,
    ext_p, ext_d, halo_p, halo_d, hsem,
    bbuf, bacc, brs, bds, bss,
    resid, sel, pick0, pick1, mixw,
    send, esem,
    xbuf, xacc, ssum, xrs, xds, xfs, xss,
    hbuf, hacc, hrs, hds, hfs, hss,
    obuf, ret, osem,
):
    s = lax.axis_index("sp")
    t = lax.axis_index("tp")
    y, c = t // 2, t % 2
    z, x = s // NX, s % NX
    nxt = (s + 1) % SP

    loads = [
        pltpu.make_async_copy(wo_hbm, wo, wsem.at[0]),
        pltpu.make_async_copy(wg_hbm, wgu.at[:, 0:CH], wsem.at[1]),
        pltpu.make_async_copy(wu_hbm, wgu.at[:, CH : 2 * CH], wsem.at[2]),
        pltpu.make_async_copy(wd_hbm, wd, wsem.at[3]),
    ]
    for load in loads:
        load.start()

    barrier = pltpu.get_barrier_semaphore()

    def greet(i, carry):
        pl.semaphore_signal(barrier, inc=1, device_id=((s + i) % SP, t), device_id_type=MESH)
        return carry

    lax.fori_loop(1, SP, greet, 0)
    for off in (1, 2, NY - 1, NY - 2):
        peer = 2 * ((y + off) % NY) + c
        pl.semaphore_signal(barrier, inc=1, device_id=(s, peer), device_id_type=MESH)
    pl.semaphore_signal(barrier, inc=1, device_id=(s, 2 * y + 1 - c), device_id_type=MESH)

    ext_p[8:264, :] = ig[...].astype(F32) * ci[...].astype(F32)
    id0, id1 = ids[0:1, :], ids[1:2, :]
    expert = lax.broadcasted_iota(jnp.int32, (SP, ROWS), 0)
    is0, is1 = expert == id0, expert == id1
    named = jnp.where(is0 | is1, 1.0, 0.0).astype(BF16)
    before = lax.broadcasted_iota(jnp.int32, (ROWS, ROWS), 0) < lax.broadcasted_iota(
        jnp.int32, (ROWS, ROWS), 1
    )
    ahead = jnp.dot(named, jnp.where(before, 1.0, 0.0).astype(BF16), preferred_element_type=F32)
    rank0 = jnp.sum(jnp.where(is0, ahead, 0.0), axis=0, keepdims=True)
    rank1 = jnp.sum(jnp.where(is1, ahead, 0.0), axis=0, keepdims=True)
    slot0 = id0.astype(F32) * CAP + rank0
    slot1 = id1.astype(F32) * CAP + rank1
    e0, e1 = ew[0:1, :], ew[1:2, :]
    esum = e0 + e1
    group = gw[...]
    table = jnp.concatenate(
        [
            docs[...].astype(F32),
            slot0,
            slot1,
            group * e0 / esum,
            group * e1 / esum,
            jnp.zeros((CH - 5, ROWS), F32),
        ],
        axis=0,
    )
    columns = table.T
    ext_d[8:264, :] = jnp.broadcast_to(columns[:, 0:1], (ROWS, CH))
    mixw[...] = columns

    taps = cw[...].astype(F32)

    def branch_rows(lo, hi):
        own_docs = ext_d[8 + lo : 8 + hi, :]
        row = lax.broadcasted_iota(jnp.int32, (hi - lo, CH), 0) + lo
        conv = taps[2:3, :] * ext_p[8 + lo : 8 + hi, :]
        for shift in (1, 2):
            rows = slice(8 + lo - shift, 8 + hi - shift)
            same = (ext_d[rows, :] == own_docs) & ((row >= shift) | (s > 0))
            conv = conv + jnp.where(same, taps[2 - shift : 3 - shift, :] * ext_p[rows, :], 0.0)
        return (og[lo:hi, :].astype(F32) * conv).astype(BF16)

    bbuf[t, 0:128, :] = branch_rows(128, 256)
    bbuf[t, 128:240, :] = branch_rows(16, 128)
    bbuf[t, 240:256, :] = jnp.concatenate(
        [gain[...].astype(F32), jnp.zeros((14, CH), F32)], axis=0
    ).astype(BF16)
    bacc[...] = jnp.zeros_like(bacc)

    pl.semaphore_wait(barrier, SP - 1 + 5)

    halos = [
        rdma(ext_p.at[256:264], halo_p, hsem.at[0], hsem.at[1], (nxt, t)),
        rdma(ext_d.at[256:264], halo_d, hsem.at[2], hsem.at[3], (nxt, t)),
    ]
    for halo in halos:
        halo.start()

    def near(off):
        return (y + off + NY) % NY

    def hop(origin, p, off):
        lo, size = BSPLIT[p]
        ref = bbuf.at[2 * origin + c, pl.ds(lo, size)]
        return rdma(ref, ref, bss, brs.at[origin, p], (s, 2 * near(off) + c))

    def across(origin, core, p):
        lo, size = BSPLIT[p]
        ref = bbuf.at[2 * origin + core, pl.ds(lo, size)]
        return rdma(ref, ref, bss, bds.at[origin, p], (s, 2 * y + 1 - c))

    def open_piece(p):
        for off in (2, -2, 1, -1):
            hop(y, p, off).start()
        across(y, c, p).start()

    open_piece(0)
    open_piece(1)
    for halo in halos:
        halo.wait_recv()
    ext_p[0:8, :] = halo_p[...]
    ext_d[0:8, :] = halo_d[...]
    bbuf[t, 256:272, :] = branch_rows(0, 16)
    open_piece(2)

    def far_side(p):
        return 1 if p != 1 else -1

    for p in range(3):
        for side in (1, -1):
            origin = near(-2 * side)
            hop(origin, p, side).wait_recv()
            if far_side(p) == side:
                hop(origin, p, 2 * side).start()
            hop(origin, p, side).start()
            across(origin, c, p).start()
        for side in (1, -1):
            origin = near(-side)
            hop(origin, p, side).wait_recv()
            across(origin, c, p).start()

    loads[0].wait()

    def project(first, count, core):
        def one(i, carry):
            chunk = 2 * ((y + first + i) % NY) + core
            weights = wo[pl.ds(pl.multiple_of(chunk * CH, CH), CH), :]
            bacc[...] += jnp.dot(bbuf[chunk], weights, preferred_element_type=F32)
            return carry

        lax.fori_loop(0, count, one, 0)

    project(6, 5, c)

    def target(q):
        dz, dx = ZORDER[q // NX], q % NX
        return ((z + dz) % NZ) * NX + (x + dx) % NX

    lane_slot = lax.broadcasted_iota(jnp.int32, (CAP, ROWS), 0)
    for q in range(SP):
        slot = (lane_slot + target(q) * CAP).astype(F32)
        sel[q * CAP : (q + 1) * CAP, :] = jnp.where(
            (slot == slot0) | (slot == slot1), 1.0, 0.0
        ).astype(BF16)

    for off in (3, -3, 4):
        origin = near(off)
        for p in range(3):
            hop(origin, p, 1).wait_recv()
            across(origin, c, p).start()
    for off in (0, 1, -1, 2, -2):
        for p in range(3):
            across(near(off), 1 - c, p).wait_recv()
    project(6, 5, 1 - c)
    project(3, 3, c)
    for off in (3, -3, 4):
        for p in range(3):
            across(near(off), 1 - c, p).wait_recv()
    project(3, 3, 1 - c)

    for (lo, size), first in zip(((0, 128), (128, 112), (256, 16)), (128, 16, 0)):
        rows = slice(first, first + size)
        resid[rows, :] = (resin[rows, :].astype(F32) + bacc[lo : lo + size, :]).astype(BF16)

    def block(ref, i):
        return ref.at[pl.ds(pl.multiple_of(i * CAP, CAP), CAP)]

    def offsets(q):
        return ZORDER[q // NX], q % NX

    for p in range(PIECES):
        rows = slice(p * PROWS, (p + 1) * PROWS)
        send[rows, :] = jnp.dot(sel[rows, :], resid[...], preferred_element_type=F32).astype(BF16)
        for q in range(p * PER, (p + 1) * PER):
            if q == 0:
                pltpu.make_async_copy(block(send, q), block(xbuf.at[t], q), esem.at[q]).start()
            else:
                dev = (target(q), t)
                rdma(block(send, q), block(xbuf.at[t], q), esem.at[SP], esem.at[q], dev).start()

    xacc[...] = jnp.zeros_like(xacc)
    ssum[...] = jnp.zeros_like(ssum)
    hacc[...] = jnp.zeros_like(hacc)
    for load in loads[1:]:
        load.wait()

    def prows(p):
        return pl.ds(pl.multiple_of(p * PROWS, PROWS), PROWS)

    def widen(chunk, p):
        rows = prows(p)
        gains = bbuf[chunk, pl.ds(240, 16), :].astype(F32)
        part = xbuf[chunk, rows, :].astype(F32)
        left, right = part[:, :CH], part[:, CH:]
        ssum[rows, :] += left * left + right * right
        scaled = jnp.concatenate([left * gains[0:1, :], right * gains[1:2, :]], axis=1).astype(BF16)
        weights = wgu[pl.ds(pl.multiple_of(chunk * COLS, COLS), COLS), :]
        xacc[rows, :] += jnp.dot(scaled, weights, preferred_element_type=F32)

    def lower(chunk, p):
        rows = prows(p)
        weights = wd[pl.ds(pl.multiple_of(chunk * CH, CH), CH), :]
        hacc[rows, :] += jnp.dot(hbuf[chunk, rows, :], weights, preferred_element_type=F32)

    slot_lane = lax.broadcasted_iota(jnp.int32, (ROWS, SLOTS), 1).astype(F32)
    pick0[...] = jnp.where(slot_lane == mixw[:, 1:2], 1.0, 0.0).astype(BF16)
    pick1[...] = jnp.where(slot_lane == mixw[:, 2:3], 1.0, 0.0).astype(BF16)

    wide = Ring(xbuf, PIECES, PROWS, xrs, xds, xfs, xss, s, y, c)
    deep = Ring(hbuf, PIECES, PROWS, hrs, hds, hfs, hss, s, y, c)

    def enter(p):
        def one(i, carry):
            q = p * PER + i
            dst = block(xbuf.at[t], q)
            pltpu.make_async_copy(dst, dst, esem.at[q]).wait()
            return carry

        lax.fori_loop(0, PER, one, 0)
        wide.begin(p)
        wide.own(p, widen)

    def activate(p):
        wide.last(p, widen)
        rows = prows(p)
        mean = jnp.sum(ssum[rows, :], axis=1, keepdims=True) / (TP * COLS)
        scale = lax.rsqrt(mean + EPS)
        gate = xacc[rows, 0:CH] * scale
        up = xacc[rows, CH : 2 * CH] * scale
        hbuf[t, rows, :] = (gate * jax.nn.sigmoid(gate) * up).astype(BF16)
        deep.begin(p)
        deep.own(p, lower)

    def leave(p):
        deep.last(p, lower)
        rows = slice(p * PROWS, (p + 1) * PROWS)
        obuf[rows, :] = hacc[rows, :].astype(BF16)
        for q in range(p * PER, (p + 1) * PER):
            dz, dx = offsets(q)
            d = ((z + NZ - dz) % NZ) * NX + (x + NX - dx) % NX
            if q == 0:
                pltpu.make_async_copy(block(obuf, q), block(ret, s), osem.at[s]).start()
            else:
                rdma(block(obuf, q), block(ret, s), osem.at[SP], osem.at[s], (d, t)).start()

    def wave(j, carry):
        p = j % PIECES
        stage = j // PIECES - p * DELAY[0] // DELAY[1]

        @pl.when((p == 0) & (j < PIECES * PIECES))
        def _():
            enter(j // PIECES)

        @pl.when((stage >= 1) & (stage <= 4))
        def _():
            wide.arrivals(stage, p, widen)

        @pl.when(stage == 5)
        def _():
            activate(p)

        @pl.when((stage >= 6) & (stage <= 9))
        def _():
            deep.arrivals(stage - 5, p, lower)

        for piece in range(PIECES):

            @pl.when((stage == 10) & (p == piece))
            def _(piece=piece):
                leave(piece)

        return carry

    lax.fori_loop(0, PIECES * (11 + (PIECES - 1) * DELAY[0] // DELAY[1]), wave, 0)

    def arrive(d, carry):
        pltpu.make_async_copy(block(ret, d), block(ret, d), osem.at[d]).wait()
        return carry

    lax.fori_loop(0, SP, arrive, 0)

    got0 = jnp.dot(pick0[...], ret[...], preferred_element_type=F32)
    got1 = jnp.dot(pick1[...], ret[...], preferred_element_type=F32)
    routed = got0 * mixw[:, 3:4] + got1 * mixw[:, 4:5]
    out[...] = resid[...].astype(F32) + routed

    for halo in halos:
        halo.wait_send()
    rest = bbuf.at[0:15]
    pltpu.make_async_copy(rest, rest, bss).wait()
    rest = send.at[0 : SLOTS - CAP]
    pltpu.make_async_copy(rest, rest, esem.at[SP]).wait()
    wide.drain()
    deep.drain()
    rest = obuf.at[0 : SLOTS - CAP]
    pltpu.make_async_copy(rest, rest, osem.at[SP]).wait()


def per_device(
    outer_gate, inner_gate, conv_input, conv_weight, doc_ids, output_weight, residual,
    norm_gain, expert_ids, group_weight, expert_weight, gate_weight, up_weight, down_weight,
):
    dma = pltpu.SemaphoreType.DMA
    vmem = pl.BlockSpec(memory_space=pltpu.VMEM)
    hbm = pl.BlockSpec(memory_space=pl.ANY)
    scratch = [
        pltpu.VMEM((TP * CH, COLS), BF16),
        pltpu.VMEM((TP * COLS, 2 * CH), BF16),
        pltpu.VMEM((TP * CH, COLS), BF16),
        dma((4,)),
        pltpu.VMEM((264, CH), F32),
        pltpu.VMEM((264, CH), F32),
        pltpu.VMEM((8, CH), F32),
        pltpu.VMEM((8, CH), F32),
        dma((4,)),
        pltpu.VMEM((TP, BROWS, CH), BF16),
        pltpu.VMEM((BROWS, COLS), F32),
        dma((NY, 3)),
        dma((NY, 3)),
        dma,
        pltpu.VMEM((ROWS, COLS), BF16),
        pltpu.VMEM((SLOTS, ROWS), BF16),
        pltpu.VMEM((ROWS, SLOTS), BF16),
        pltpu.VMEM((ROWS, SLOTS), BF16),
        pltpu.VMEM((ROWS, CH), F32),
        pltpu.VMEM((SLOTS, COLS), BF16),
        dma((SP + 1,)),
        pltpu.VMEM((TP, SLOTS, COLS), BF16),
        pltpu.VMEM((SLOTS, 2 * CH), F32),
        pltpu.VMEM((SLOTS, CH), F32),
        dma((NY, PIECES)),
        dma((NY, PIECES)),
        dma((2, PIECES)),
        dma,
        pltpu.VMEM((TP, SLOTS, CH), BF16),
        pltpu.VMEM((SLOTS, COLS), F32),
        dma((NY, PIECES)),
        dma((NY, PIECES)),
        dma((2, PIECES)),
        dma,
        pltpu.VMEM((SLOTS, COLS), BF16),
        pltpu.VMEM((SLOTS, COLS), BF16),
        dma((SP + 1,)),
    ]
    return pl.pallas_call(
        kernel,
        name="layer",
        out_shape=jax.ShapeDtypeStruct((ROWS, COLS), F32),
        in_specs=[vmem] * 10 + [hbm] * 4,
        out_specs=vmem,
        scratch_shapes=scratch,
        compiler_params=pltpu.CompilerParams(
            collective_id=0, has_side_effects=True, vmem_limit_bytes=56 * 1024 * 1024
        ),
    )(
        outer_gate,
        inner_gate,
        conv_input,
        conv_weight,
        doc_ids.reshape(1, ROWS),
        residual,
        norm_gain.reshape(2, CH),
        expert_ids.T,
        group_weight.reshape(1, ROWS),
        expert_weight.T,
        output_weight,
        gate_weight[0],
        up_weight[0],
        down_weight[0],
    ).astype(BF16)


def solution(mesh):
    return jax.shard_map(
        per_device,
        mesh=mesh,
        in_specs=(
            P("sp", "tp"),
            P("sp", "tp"),
            P("sp", "tp"),
            P(None, "tp"),
            P("sp"),
            P(None, "tp"),
            P("sp", "tp"),
            P("tp"),
            P("sp", None),
            P("sp"),
            P("sp", None),
            P("sp", None, "tp"),
            P("sp", None, "tp"),
            P("sp", None, "tp"),
        ),
        out_specs=P("sp", "tp"),
        check_vma=False,
    )
```

```python
import functools
import jax
import jax.numpy as jnp
from jax import lax
from jax.experimental import pallas as pl
from jax.experimental.pallas import tpu as pltpu
from jax.sharding import PartitionSpec as P

EPS = 1e-06
MESH = pl.DeviceIdType.MESH
F32 = jnp.float32
BF16 = jnp.bfloat16

SP, NX, NZ = 32, 4, 8
TP, NY = 16, 8
ROWS = 256
COLS = 256
CH = 128
CAP = 32
SLOTS = SP * CAP
PIECES = 4
PROWS = SLOTS // PIECES
PER = SP // PIECES
DELAY = (1, 1)
ZORDER = (0, 1, 6, 3, 5, 4, 7, 2)
BROWS = 272
BSPLIT = ((0, 128), (128, 128), (256, 16))


def rdma(src, dst, ssem, rsem, dev):
    return pltpu.make_async_remote_copy(
        src_ref=src, dst_ref=dst, send_sem=ssem, recv_sem=rsem, device_id=dev, device_id_type=MESH
    )


class Ring:
    def __init__(self, buf, pieces, prows, rsem, dsem, fsem, ssem, s, y, c):
        self.buf, self.pieces, self.prows = buf, pieces, prows
        self.rsem, self.dsem, self.fsem, self.ssem = rsem, dsem, fsem, ssem
        self.s, self.y, self.c = s, y, c
        self.plus = (s, 2 * ((y + 1) % NY) + c)
        self.minus = (s, 2 * ((y + NY - 1) % NY) + c)
        self.partner = (s, 2 * y + (1 - c))

    def at(self, chunk, p):
        return self.buf.at[chunk, pl.ds(pl.multiple_of(p * self.prows, 16), self.prows)]

    def ring(self, origin, p, dev):
        ref = self.at(2 * origin + self.c, p)
        return rdma(ref, ref, self.ssem, self.rsem.at[origin, p], dev)

    def local(self, origin, core, p):
        ref = self.at(2 * origin + core, p)
        return rdma(ref, ref, self.ssem, self.dsem.at[origin, p], self.partner)

    def begin(self, p):
        self.ring(self.y, p, self.plus).start()
        self.ring(self.y, p, self.minus).start()
        self.local(self.y, self.c, p).start()

    def own(self, p, compute):
        compute(2 * self.y + self.c, p)

    def half(self, p, h, dev):
        rows = self.prows // 2
        far = self.buf.at[
            2 * h[0] + self.c, pl.ds(pl.multiple_of(p * self.prows + h[1] * rows, 16), rows)
        ]
        return rdma(far, far, self.ssem, self.fsem.at[h[1], p], dev)

    def arrivals(self, k, p, compute):
        up = (self.y + NY - k) % NY
        down = (self.y + k) % NY
        c = self.c

        @pl.when(k < 4)
        def _():
            for origin, side, h in ((up, self.plus, 0), (down, self.minus, 1)):
                self.ring(origin, p, side).wait_recv()

                @pl.when(k < 3)
                def _():
                    self.ring(origin, p, side).start()

                @pl.when(k == 3)
                def _():
                    self.half(p, (origin, h), side).start()

                self.local(origin, c, p).start()

        @pl.when(k == 4)
        def _():
            for h in (0, 1):
                self.half(p, (up, h), self.plus).wait_recv()
            self.local(up, c, p).start()

        compute(2 * up + c, p)

        @pl.when(k < 4)
        def _():
            compute(2 * down + c, p)

        pup = (self.y + NY - (k - 1)) % NY
        pdown = (self.y + (k - 1)) % NY
        self.local(pup, 1 - c, p).wait_recv()
        compute(2 * pup + 1 - c, p)

        @pl.when(k > 1)
        def _():
            self.local(pdown, 1 - c, p).wait_recv()
            compute(2 * pdown + 1 - c, p)

    def last(self, p, compute):
        far = (self.y + 4) % NY
        self.local(far, 1 - self.c, p).wait_recv()
        compute(2 * far + 1 - self.c, p)

    def drain(self):
        ref = self.buf.at[0:15]
        pltpu.make_async_copy(ref, ref, self.ssem).wait()


def kernel(
    og, ig, ci, cw, docs, resin, gain, ids, gw, ew, wo_hbm, wg_hbm, wu_hbm, wd_hbm,
    out,
    wo, wgu, wd, wsem,
    ext_p, ext_d, halo_p, halo_d, hsem,
    bbuf, bacc, brs, bds, bss,
    resid, sel, pick0, pick1, mixw,
    send, esem,
    xbuf, xacc, ssum, xrs, xds, xfs, xss,
    hbuf, hacc, hrs, hds, hfs, hss,
    obuf, ret, osem,
):
    s = lax.axis_index("sp")
    t = lax.axis_index("tp")
    y, c = t // 2, t % 2
    z, x = s // NX, s % NX
    nxt = (s + 1) % SP

    loads = [
        pltpu.make_async_copy(wo_hbm, wo, wsem.at[0]),
        pltpu.make_async_copy(wg_hbm, wgu.at[:, 0:CH], wsem.at[1]),
        pltpu.make_async_copy(wu_hbm, wgu.at[:, CH : 2 * CH], wsem.at[2]),
        pltpu.make_async_copy(wd_hbm, wd, wsem.at[3]),
    ]
    for load in loads:
        load.start()

    barrier = pltpu.get_barrier_semaphore()

    def greet(i, carry):
        pl.semaphore_signal(barrier, inc=1, device_id=((s + i) % SP, t), device_id_type=MESH)
        return carry

    lax.fori_loop(1, SP, greet, 0)
    for off in range(1, NY):
        peer = 2 * ((y + off) % NY) + c
        pl.semaphore_signal(barrier, inc=1, device_id=(s, peer), device_id_type=MESH)
    pl.semaphore_signal(barrier, inc=1, device_id=(s, 2 * y + 1 - c), device_id_type=MESH)

    ext_p[8:264, :] = ig[...].astype(F32) * ci[...].astype(F32)
    id0, id1 = ids[0:1, :], ids[1:2, :]
    expert = lax.broadcasted_iota(jnp.int32, (SP, ROWS), 0)
    is0, is1 = expert == id0, expert == id1
    named = jnp.where(is0 | is1, 1.0, 0.0).astype(BF16)
    before = lax.broadcasted_iota(jnp.int32, (ROWS, ROWS), 0) < lax.broadcasted_iota(
        jnp.int32, (ROWS, ROWS), 1
    )
    ahead = jnp.dot(named, jnp.where(before, 1.0, 0.0).astype(BF16), preferred_element_type=F32)
    rank0 = jnp.sum(jnp.where(is0, ahead, 0.0), axis=0, keepdims=True)
    rank1 = jnp.sum(jnp.where(is1, ahead, 0.0), axis=0, keepdims=True)
    slot0 = id0.astype(F32) * CAP + rank0
    slot1 = id1.astype(F32) * CAP + rank1
    e0, e1 = ew[0:1, :], ew[1:2, :]
    esum = e0 + e1
    group = gw[...]
    table = jnp.concatenate(
        [
            docs[...].astype(F32),
            slot0,
            slot1,
            group * e0 / esum,
            group * e1 / esum,
            jnp.zeros((CH - 5, ROWS), F32),
        ],
        axis=0,
    )
    columns = table.T
    ext_d[8:264, :] = jnp.broadcast_to(columns[:, 0:1], (ROWS, CH))
    mixw[...] = columns

    taps = cw[...].astype(F32)

    def branch_rows(lo, hi):
        own_docs = ext_d[8 + lo : 8 + hi, :]
        row = lax.broadcasted_iota(jnp.int32, (hi - lo, CH), 0) + lo
        conv = taps[2:3, :] * ext_p[8 + lo : 8 + hi, :]
        for shift in (1, 2):
            rows = slice(8 + lo - shift, 8 + hi - shift)
            same = (ext_d[rows, :] == own_docs) & ((row >= shift) | (s > 0))
            conv = conv + jnp.where(same, taps[2 - shift : 3 - shift, :] * ext_p[rows, :], 0.0)
        return (og[lo:hi, :].astype(F32) * conv).astype(BF16)

    bbuf[t, 0:128, :] = branch_rows(128, 256)
    bbuf[t, 128:240, :] = branch_rows(16, 128)
    bbuf[t, 240:256, :] = jnp.concatenate(
        [gain[...].astype(F32), jnp.zeros((14, CH), F32)], axis=0
    ).astype(BF16)
    bacc[...] = jnp.zeros_like(bacc)

    pl.semaphore_wait(barrier, SP - 1 + NY)

    halos = [
        rdma(ext_p.at[256:264], halo_p, hsem.at[0], hsem.at[1], (nxt, t)),
        rdma(ext_d.at[256:264], halo_d, hsem.at[2], hsem.at[3], (nxt, t)),
    ]
    for halo in halos:
        halo.start()

    def near(off):
        return (y + off + NY) % NY

    def hop(origin, p, off):
        lo, size = BSPLIT[p]
        ref = bbuf.at[2 * origin + c, pl.ds(lo, size)]
        return rdma(ref, ref, bss, brs.at[origin, p], (s, 2 * near(off) + c))

    def across(origin, core, p):
        lo, size = BSPLIT[p]
        ref = bbuf.at[2 * origin + core, pl.ds(lo, size)]
        return rdma(ref, ref, bss, bds.at[origin, p], (s, 2 * y + 1 - c))

    def open_piece(p):
        for off in (2, -2, 1, -1) if p < 2 else (4, 3, -3, 2, -2, 1, -1):
            hop(y, p, off).start()
        across(y, c, p).start()

    open_piece(0)
    open_piece(1)
    for halo in halos:
        halo.wait_recv()
    ext_p[0:8, :] = halo_p[...]
    ext_d[0:8, :] = halo_d[...]
    bbuf[t, 256:272, :] = branch_rows(0, 16)
    open_piece(2)

    def far_side(p):
        return 1 if p == 0 else -1

    for p in range(3):
        for side in (1, -1):
            origin = near(-2 * side)
            hop(origin, p, side).wait_recv()
            if p < 2:
                if far_side(p) == side:
                    hop(origin, p, 2 * side).start()
                hop(origin, p, side).start()
            across(origin, c, p).start()
        for side in (1, -1):
            origin = near(-side)
            hop(origin, p, side).wait_recv()
            across(origin, c, p).start()

    loads[0].wait()

    def project(first, count, core):
        def one(i, carry):
            chunk = 2 * ((y + first + i) % NY) + core
            weights = wo[pl.ds(pl.multiple_of(chunk * CH, CH), CH), :]
            bacc[...] += jnp.dot(bbuf[chunk], weights, preferred_element_type=F32)
            return carry

        lax.fori_loop(0, count, one, 0)

    project(6, 5, c)

    def target(q):
        dz, dx = ZORDER[q // NX], q % NX
        return ((z + dz) % NZ) * NX + (x + dx) % NX

    lane_slot = lax.broadcasted_iota(jnp.int32, (CAP, ROWS), 0)
    for q in range(SP):
        slot = (lane_slot + target(q) * CAP).astype(F32)
        sel[q * CAP : (q + 1) * CAP, :] = jnp.where(
            (slot == slot0) | (slot == slot1), 1.0, 0.0
        ).astype(BF16)

    for off in (3, -3, 4):
        origin = near(off)
        for p in range(3):
            hop(origin, p, 1).wait_recv()
            across(origin, c, p).start()
    for off in (0, 1, -1, 2, -2):
        for p in range(3):
            across(near(off), 1 - c, p).wait_recv()
    project(6, 5, 1 - c)
    project(3, 3, c)
    for off in (3, -3, 4):
        for p in range(3):
            across(near(off), 1 - c, p).wait_recv()
    project(3, 3, 1 - c)

    for (lo, size), first in zip(((0, 128), (128, 112), (256, 16)), (128, 16, 0)):
        rows = slice(first, first + size)
        resid[rows, :] = (resin[rows, :].astype(F32) + bacc[lo : lo + size, :]).astype(BF16)

    def block(ref, i):
        return ref.at[pl.ds(pl.multiple_of(i * CAP, CAP), CAP)]

    def offsets(q):
        return ZORDER[q // NX], q % NX

    for p in range(PIECES):
        rows = slice(p * PROWS, (p + 1) * PROWS)
        send[rows, :] = jnp.dot(sel[rows, :], resid[...], preferred_element_type=F32).astype(BF16)
        for q in range(p * PER, (p + 1) * PER):
            if q == 0:
                pltpu.make_async_copy(block(send, q), block(xbuf.at[t], q), esem.at[q]).start()
            else:
                dev = (target(q), t)
                rdma(block(send, q), block(xbuf.at[t], q), esem.at[SP], esem.at[q], dev).start()

    xacc[...] = jnp.zeros_like(xacc)
    ssum[...] = jnp.zeros_like(ssum)
    hacc[...] = jnp.zeros_like(hacc)
    for load in loads[1:]:
        load.wait()

    def prows(p):
        return pl.ds(pl.multiple_of(p * PROWS, PROWS), PROWS)

    def widen(chunk, p):
        rows = prows(p)
        gains = bbuf[chunk, pl.ds(240, 16), :].astype(F32)
        part = xbuf[chunk, rows, :].astype(F32)
        left, right = part[:, :CH], part[:, CH:]
        ssum[rows, :] += left * left + right * right
        scaled = jnp.concatenate([left * gains[0:1, :], right * gains[1:2, :]], axis=1).astype(BF16)
        weights = wgu[pl.ds(pl.multiple_of(chunk * COLS, COLS), COLS), :]
        xacc[rows, :] += jnp.dot(scaled, weights, preferred_element_type=F32)

    def lower(chunk, p):
        rows = prows(p)
        weights = wd[pl.ds(pl.multiple_of(chunk * CH, CH), CH), :]
        hacc[rows, :] += jnp.dot(hbuf[chunk, rows, :], weights, preferred_element_type=F32)

    slot_lane = lax.broadcasted_iota(jnp.int32, (ROWS, SLOTS), 1).astype(F32)
    pick0[...] = jnp.where(slot_lane == mixw[:, 1:2], 1.0, 0.0).astype(BF16)
    pick1[...] = jnp.where(slot_lane == mixw[:, 2:3], 1.0, 0.0).astype(BF16)

    wide = Ring(xbuf, PIECES, PROWS, xrs, xds, xfs, xss, s, y, c)
    deep = Ring(hbuf, PIECES, PROWS, hrs, hds, hfs, hss, s, y, c)

    def enter(p):
        def one(i, carry):
            q = p * PER + i
            dst = block(xbuf.at[t], q)
            pltpu.make_async_copy(dst, dst, esem.at[q]).wait()
            return carry

        lax.fori_loop(0, PER, one, 0)
        wide.begin(p)
        wide.own(p, widen)

    def activate(p):
        wide.last(p, widen)
        rows = prows(p)
        mean = jnp.sum(ssum[rows, :], axis=1, keepdims=True) / (TP * COLS)
        scale = lax.rsqrt(mean + EPS)
        gate = xacc[rows, 0:CH] * scale
        up = xacc[rows, CH : 2 * CH] * scale
        hbuf[t, rows, :] = (gate * jax.nn.sigmoid(gate) * up).astype(BF16)
        deep.begin(p)
        deep.own(p, lower)

    def leave(p):
        deep.last(p, lower)
        rows = slice(p * PROWS, (p + 1) * PROWS)
        obuf[rows, :] = hacc[rows, :].astype(BF16)
        for q in range(p * PER, (p + 1) * PER):
            dz, dx = offsets(q)
            d = ((z + NZ - dz) % NZ) * NX + (x + NX - dx) % NX
            if q == 0:
                pltpu.make_async_copy(block(obuf, q), block(ret, s), osem.at[s]).start()
            else:
                rdma(block(obuf, q), block(ret, s), osem.at[SP], osem.at[s], (d, t)).start()

    def wave(j, carry):
        p = j % PIECES
        stage = j // PIECES - p * DELAY[0] // DELAY[1]

        @pl.when((p == 0) & (j < PIECES * PIECES))
        def _():
            enter(j // PIECES)

        @pl.when((stage >= 1) & (stage <= 4))
        def _():
            wide.arrivals(stage, p, widen)

        @pl.when(stage == 5)
        def _():
            activate(p)

        @pl.when((stage >= 6) & (stage <= 9))
        def _():
            deep.arrivals(stage - 5, p, lower)

        for piece in range(PIECES):

            @pl.when((stage == 10) & (p == piece))
            def _(piece=piece):
                leave(piece)

        return carry

    lax.fori_loop(0, PIECES * (11 + (PIECES - 1) * DELAY[0] // DELAY[1]), wave, 0)

    def arrive(d, carry):
        pltpu.make_async_copy(block(ret, d), block(ret, d), osem.at[d]).wait()
        return carry

    lax.fori_loop(0, SP, arrive, 0)

    got0 = jnp.dot(pick0[...], ret[...], preferred_element_type=F32)
    got1 = jnp.dot(pick1[...], ret[...], preferred_element_type=F32)
    routed = got0 * mixw[:, 3:4] + got1 * mixw[:, 4:5]
    out[...] = resid[...].astype(F32) + routed

    for halo in halos:
        halo.wait_send()
    rest = bbuf.at[0:15]
    pltpu.make_async_copy(rest, rest, bss).wait()
    rest = send.at[0 : SLOTS - CAP]
    pltpu.make_async_copy(rest, rest, esem.at[SP]).wait()
    wide.drain()
    deep.drain()
    rest = obuf.at[0 : SLOTS - CAP]
    pltpu.make_async_copy(rest, rest, osem.at[SP]).wait()


def per_device(
    outer_gate, inner_gate, conv_input, conv_weight, doc_ids, output_weight, residual,
    norm_gain, expert_ids, group_weight, expert_weight, gate_weight, up_weight, down_weight,
):
    dma = pltpu.SemaphoreType.DMA
    vmem = pl.BlockSpec(memory_space=pltpu.VMEM)
    hbm = pl.BlockSpec(memory_space=pl.ANY)
    scratch = [
        pltpu.VMEM((TP * CH, COLS), BF16),
        pltpu.VMEM((TP * COLS, 2 * CH), BF16),
        pltpu.VMEM((TP * CH, COLS), BF16),
        dma((4,)),
        pltpu.VMEM((264, CH), F32),
        pltpu.VMEM((264, CH), F32),
        pltpu.VMEM((8, CH), F32),
        pltpu.VMEM((8, CH), F32),
        dma((4,)),
        pltpu.VMEM((TP, BROWS, CH), BF16),
        pltpu.VMEM((BROWS, COLS), F32),
        dma((NY, 3)),
        dma((NY, 3)),
        dma,
        pltpu.VMEM((ROWS, COLS), BF16),
        pltpu.VMEM((SLOTS, ROWS), BF16),
        pltpu.VMEM((ROWS, SLOTS), BF16),
        pltpu.VMEM((ROWS, SLOTS), BF16),
        pltpu.VMEM((ROWS, CH), F32),
        pltpu.VMEM((SLOTS, COLS), BF16),
        dma((SP + 1,)),
        pltpu.VMEM((TP, SLOTS, COLS), BF16),
        pltpu.VMEM((SLOTS, 2 * CH), F32),
        pltpu.VMEM((SLOTS, CH), F32),
        dma((NY, PIECES)),
        dma((NY, PIECES)),
        dma((2, PIECES)),
        dma,
        pltpu.VMEM((TP, SLOTS, CH), BF16),
        pltpu.VMEM((SLOTS, COLS), F32),
        dma((NY, PIECES)),
        dma((NY, PIECES)),
        dma((2, PIECES)),
        dma,
        pltpu.VMEM((SLOTS, COLS), BF16),
        pltpu.VMEM((SLOTS, COLS), BF16),
        dma((SP + 1,)),
    ]
    return pl.pallas_call(
        kernel,
        name="layer",
        out_shape=jax.ShapeDtypeStruct((ROWS, COLS), F32),
        in_specs=[vmem] * 10 + [hbm] * 4,
        out_specs=vmem,
        scratch_shapes=scratch,
        compiler_params=pltpu.CompilerParams(
            collective_id=0, has_side_effects=True, vmem_limit_bytes=56 * 1024 * 1024
        ),
    )(
        outer_gate,
        inner_gate,
        conv_input,
        conv_weight,
        doc_ids.reshape(1, ROWS),
        residual,
        norm_gain.reshape(2, CH),
        expert_ids.T,
        group_weight.reshape(1, ROWS),
        expert_weight.T,
        output_weight,
        gate_weight[0],
        up_weight[0],
        down_weight[0],
    ).astype(BF16)


def solution(mesh):
    return jax.shard_map(
        per_device,
        mesh=mesh,
        in_specs=(
            P("sp", "tp"),
            P("sp", "tp"),
            P("sp", "tp"),
            P(None, "tp"),
            P("sp"),
            P(None, "tp"),
            P("sp", "tp"),
            P("tp"),
            P("sp", None),
            P("sp"),
            P("sp", None),
            P("sp", None, "tp"),
            P("sp", None, "tp"),
            P("sp", None, "tp"),
        ),
        out_specs=P("sp", "tp"),
        check_vma=False,
    )
```

```python
import functools
import jax
import jax.numpy as jnp
from jax import lax
from jax.experimental import pallas as pl
from jax.experimental.pallas import tpu as pltpu
from jax.sharding import PartitionSpec as P

EPS = 1e-06
MESH = pl.DeviceIdType.MESH
F32 = jnp.float32
BF16 = jnp.bfloat16

SP, NX, NZ = 32, 4, 8
TP, NY = 16, 8
ROWS = 256
COLS = 256
CH = 128
CAP = 32
SLOTS = SP * CAP
PIECES = 4
PROWS = SLOTS // PIECES
PER = SP // PIECES
DELAY = (1, 1)
ZORDER = (0, 1, 6, 3, 5, 4, 7, 2)
BROWS = 272
BSPLIT = ((0, 128), (128, 128), (256, 16))


def rdma(src, dst, ssem, rsem, dev):
    return pltpu.make_async_remote_copy(
        src_ref=src, dst_ref=dst, send_sem=ssem, recv_sem=rsem, device_id=dev, device_id_type=MESH
    )


class Ring:
    def __init__(self, buf, pieces, prows, rsem, dsem, fsem, ssem, s, y, c):
        self.buf, self.pieces, self.prows = buf, pieces, prows
        self.rsem, self.dsem, self.fsem, self.ssem = rsem, dsem, fsem, ssem
        self.s, self.y, self.c = s, y, c
        self.plus = (s, 2 * ((y + 1) % NY) + c)
        self.minus = (s, 2 * ((y + NY - 1) % NY) + c)
        self.partner = (s, 2 * y + (1 - c))

    def at(self, chunk, p):
        return self.buf.at[chunk, pl.ds(pl.multiple_of(p * self.prows, 16), self.prows)]

    def ring(self, origin, p, dev):
        ref = self.at(2 * origin + self.c, p)
        return rdma(ref, ref, self.ssem, self.rsem.at[origin, p], dev)

    def local(self, origin, core, p):
        ref = self.at(2 * origin + core, p)
        return rdma(ref, ref, self.ssem, self.dsem.at[origin, p], self.partner)

    def begin(self, p):
        self.ring(self.y, p, self.plus).start()
        self.ring(self.y, p, self.minus).start()
        self.local(self.y, self.c, p).start()

    def own(self, p, compute):
        compute(2 * self.y + self.c, p)

    def half(self, p, h, dev):
        rows = self.prows // 2
        far = self.buf.at[
            2 * h[0] + self.c, pl.ds(pl.multiple_of(p * self.prows + h[1] * rows, 16), rows)
        ]
        return rdma(far, far, self.ssem, self.fsem.at[h[1], p], dev)

    def arrivals(self, k, p, compute):
        up = (self.y + NY - k) % NY
        down = (self.y + k) % NY
        c = self.c

        @pl.when(k < 4)
        def _():
            for origin, side, h in ((up, self.plus, 0), (down, self.minus, 1)):
                self.ring(origin, p, side).wait_recv()

                @pl.when(k < 3)
                def _():
                    self.ring(origin, p, side).start()

                @pl.when(k == 3)
                def _():
                    self.half(p, (origin, h), side).start()

                self.local(origin, c, p).start()

        @pl.when(k == 4)
        def _():
            for h in (0, 1):
                self.half(p, (up, h), self.plus).wait_recv()
            self.local(up, c, p).start()

        compute(2 * up + c, p)

        @pl.when(k < 4)
        def _():
            compute(2 * down + c, p)

        pup = (self.y + NY - (k - 1)) % NY
        pdown = (self.y + (k - 1)) % NY
        self.local(pup, 1 - c, p).wait_recv()
        compute(2 * pup + 1 - c, p)

        @pl.when(k > 1)
        def _():
            self.local(pdown, 1 - c, p).wait_recv()
            compute(2 * pdown + 1 - c, p)

    def last(self, p, compute):
        far = (self.y + 4) % NY
        self.local(far, 1 - self.c, p).wait_recv()
        compute(2 * far + 1 - self.c, p)

    def drain(self):
        ref = self.buf.at[0:15]
        pltpu.make_async_copy(ref, ref, self.ssem).wait()


def kernel(
    og, ig, ci, cw, docs, resin, gain, ids, gw, ew, wo_hbm, wg_hbm, wu_hbm, wd_hbm,
    out,
    wo, wgu, wd, wsem,
    ext_p, ext_d, halo_p, halo_d, hsem,
    bbuf, bacc, brs, bds, bss,
    resid, sel, pick0, pick1, mixw,
    send, esem,
    xbuf, xacc, ssum, xrs, xds, xfs, xss,
    hbuf, hacc, hrs, hds, hfs, hss,
    obuf, ret, osem,
):
    s = lax.axis_index("sp")
    t = lax.axis_index("tp")
    y, c = t // 2, t % 2
    z, x = s // NX, s % NX
    nxt = (s + 1) % SP

    loads = [
        pltpu.make_async_copy(wo_hbm, wo, wsem.at[0]),
        pltpu.make_async_copy(wg_hbm, wgu.at[:, 0:CH], wsem.at[1]),
        pltpu.make_async_copy(wu_hbm, wgu.at[:, CH : 2 * CH], wsem.at[2]),
        pltpu.make_async_copy(wd_hbm, wd, wsem.at[3]),
    ]
    for load in loads:
        load.start()

    barrier = pltpu.get_barrier_semaphore()

    def greet(i, carry):
        pl.semaphore_signal(barrier, inc=1, device_id=((s + i) % SP, t), device_id_type=MESH)
        return carry

    lax.fori_loop(1, SP, greet, 0)
    for off in range(1, NY):
        peer = 2 * ((y + off) % NY) + c
        pl.semaphore_signal(barrier, inc=1, device_id=(s, peer), device_id_type=MESH)
    pl.semaphore_signal(barrier, inc=1, device_id=(s, 2 * y + 1 - c), device_id_type=MESH)

    ext_p[8:264, :] = ig[...].astype(F32) * ci[...].astype(F32)
    id0, id1 = ids[0:1, :], ids[1:2, :]
    expert = lax.broadcasted_iota(jnp.int32, (SP, ROWS), 0)
    is0, is1 = expert == id0, expert == id1
    named = jnp.where(is0 | is1, 1.0, 0.0).astype(BF16)
    before = lax.broadcasted_iota(jnp.int32, (ROWS, ROWS), 0) < lax.broadcasted_iota(
        jnp.int32, (ROWS, ROWS), 1
    )
    ahead = jnp.dot(named, jnp.where(before, 1.0, 0.0).astype(BF16), preferred_element_type=F32)
    rank0 = jnp.sum(jnp.where(is0, ahead, 0.0), axis=0, keepdims=True)
    rank1 = jnp.sum(jnp.where(is1, ahead, 0.0), axis=0, keepdims=True)
    slot0 = id0.astype(F32) * CAP + rank0
    slot1 = id1.astype(F32) * CAP + rank1
    e0, e1 = ew[0:1, :], ew[1:2, :]
    esum = e0 + e1
    group = gw[...]
    table = jnp.concatenate(
        [
            docs[...].astype(F32),
            slot0,
            slot1,
            group * e0 / esum,
            group * e1 / esum,
            jnp.zeros((CH - 5, ROWS), F32),
        ],
        axis=0,
    )
    columns = table.T
    ext_d[8:264, :] = jnp.broadcast_to(columns[:, 0:1], (ROWS, CH))
    mixw[...] = columns

    taps = cw[...].astype(F32)

    def branch_rows(lo, hi):
        own_docs = ext_d[8 + lo : 8 + hi, :]
        row = lax.broadcasted_iota(jnp.int32, (hi - lo, CH), 0) + lo
        conv = taps[2:3, :] * ext_p[8 + lo : 8 + hi, :]
        for shift in (1, 2):
            rows = slice(8 + lo - shift, 8 + hi - shift)
            same = (ext_d[rows, :] == own_docs) & ((row >= shift) | (s > 0))
            conv = conv + jnp.where(same, taps[2 - shift : 3 - shift, :] * ext_p[rows, :], 0.0)
        return (og[lo:hi, :].astype(F32) * conv).astype(BF16)

    bbuf[t, 0:128, :] = branch_rows(128, 256)
    bbuf[t, 128:240, :] = branch_rows(16, 128)
    bbuf[t, 240:256, :] = jnp.concatenate(
        [gain[...].astype(F32), jnp.zeros((14, CH), F32)], axis=0
    ).astype(BF16)
    bacc[...] = jnp.zeros_like(bacc)

    pl.semaphore_wait(barrier, SP - 1 + NY)

    halos = [
        rdma(ext_p.at[256:264], halo_p, hsem.at[0], hsem.at[1], (nxt, t)),
        rdma(ext_d.at[256:264], halo_d, hsem.at[2], hsem.at[3], (nxt, t)),
    ]
    for halo in halos:
        halo.start()

    def near(off):
        return (y + off + NY) % NY

    def hop(origin, p, off):
        lo, size = BSPLIT[p]
        ref = bbuf.at[2 * origin + c, pl.ds(lo, size)]
        return rdma(ref, ref, bss, brs.at[origin, p], (s, 2 * near(off) + c))

    def across(origin, core, p):
        lo, size = BSPLIT[p]
        ref = bbuf.at[2 * origin + core, pl.ds(lo, size)]
        return rdma(ref, ref, bss, bds.at[origin, p], (s, 2 * y + 1 - c))

    def open_piece(p):
        for off in (2, -2, 1, -1) if p < 2 else (4, 3, -3, 2, -2, 1, -1):
            hop(y, p, off).start()
        across(y, c, p).start()

    open_piece(0)
    open_piece(1)
    for halo in halos:
        halo.wait_recv()
    ext_p[0:8, :] = halo_p[...]
    ext_d[0:8, :] = halo_d[...]
    bbuf[t, 256:272, :] = branch_rows(0, 16)
    open_piece(2)

    def far_side(p):
        return 1 if p == 0 else -1

    for p in range(3):
        for side in (1, -1):
            origin = near(-2 * side)
            hop(origin, p, side).wait_recv()
            if p < 2:
                if far_side(p) == side:
                    hop(origin, p, 2 * side).start()
                hop(origin, p, side).start()
            across(origin, c, p).start()
        for side in (1, -1):
            origin = near(-side)
            hop(origin, p, side).wait_recv()
            across(origin, c, p).start()

    loads[0].wait()

    def project(first, count, core):
        def one(i, carry):
            chunk = 2 * ((y + first + i) % NY) + core
            weights = wo[pl.ds(pl.multiple_of(chunk * CH, CH), CH), :]
            bacc[...] += jnp.dot(bbuf[chunk], weights, preferred_element_type=F32)
            return carry

        lax.fori_loop(0, count, one, 0)

    project(6, 5, c)

    def target(q):
        dz, dx = ZORDER[q // NX], q % NX
        return ((z + dz) % NZ) * NX + (x + dx) % NX

    lane_slot = lax.broadcasted_iota(jnp.int32, (CAP, ROWS), 0)
    for q in range(SP):
        slot = (lane_slot + target(q) * CAP).astype(F32)
        sel[q * CAP : (q + 1) * CAP, :] = jnp.where(
            (slot == slot0) | (slot == slot1), 1.0, 0.0
        ).astype(BF16)

    for off in (3, -3, 4):
        origin = near(off)
        for p in range(3):
            hop(origin, p, 1).wait_recv()
            across(origin, c, p).start()
    for off in (0, 1, -1, 2, -2):
        for p in range(3):
            across(near(off), 1 - c, p).wait_recv()
    project(6, 5, 1 - c)
    project(3, 3, c)
    for off in (3, -3, 4):
        for p in range(3):
            across(near(off), 1 - c, p).wait_recv()
    project(3, 3, 1 - c)

    for (lo, size), first in zip(((0, 128), (128, 112), (256, 16)), (128, 16, 0)):
        rows = slice(first, first + size)
        resid[rows, :] = (resin[rows, :].astype(F32) + bacc[lo : lo + size, :]).astype(BF16)

    def block(ref, i):
        return ref.at[pl.ds(pl.multiple_of(i * CAP, CAP), CAP)]

    def offsets(q):
        return ZORDER[q // NX], q % NX

    def hops(q):
        dz, dx = offsets(q)
        return min(dz, NZ - dz) + min(dx, NX - dx)

    def far_first(p):
        return sorted(range(p * PER, (p + 1) * PER), key=lambda q: (-hops(q), q))

    for p in range(PIECES):
        rows = slice(p * PROWS, (p + 1) * PROWS)
        send[rows, :] = jnp.dot(sel[rows, :], resid[...], preferred_element_type=F32).astype(BF16)
        for q in far_first(p):
            if q == 0:
                pltpu.make_async_copy(block(send, q), block(xbuf.at[t], q), esem.at[q]).start()
            else:
                dev = (target(q), t)
                rdma(block(send, q), block(xbuf.at[t], q), esem.at[SP], esem.at[q], dev).start()

    xacc[...] = jnp.zeros_like(xacc)
    ssum[...] = jnp.zeros_like(ssum)
    hacc[...] = jnp.zeros_like(hacc)
    for load in loads[1:]:
        load.wait()

    def prows(p):
        return pl.ds(pl.multiple_of(p * PROWS, PROWS), PROWS)

    def widen(chunk, p):
        rows = prows(p)
        gains = bbuf[chunk, pl.ds(240, 16), :].astype(F32)
        part = xbuf[chunk, rows, :].astype(F32)
        left, right = part[:, :CH], part[:, CH:]
        ssum[rows, :] += left * left + right * right
        scaled = jnp.concatenate([left * gains[0:1, :], right * gains[1:2, :]], axis=1).astype(BF16)
        weights = wgu[pl.ds(pl.multiple_of(chunk * COLS, COLS), COLS), :]
        xacc[rows, :] += jnp.dot(scaled, weights, preferred_element_type=F32)

    def lower(chunk, p):
        rows = prows(p)
        weights = wd[pl.ds(pl.multiple_of(chunk * CH, CH), CH), :]
        hacc[rows, :] += jnp.dot(hbuf[chunk, rows, :], weights, preferred_element_type=F32)

    slot_lane = lax.broadcasted_iota(jnp.int32, (ROWS, SLOTS), 1).astype(F32)
    pick0[...] = jnp.where(slot_lane == mixw[:, 1:2], 1.0, 0.0).astype(BF16)
    pick1[...] = jnp.where(slot_lane == mixw[:, 2:3], 1.0, 0.0).astype(BF16)

    wide = Ring(xbuf, PIECES, PROWS, xrs, xds, xfs, xss, s, y, c)
    deep = Ring(hbuf, PIECES, PROWS, hrs, hds, hfs, hss, s, y, c)

    def enter(p):
        def one(i, carry):
            q = p * PER + i
            dst = block(xbuf.at[t], q)
            pltpu.make_async_copy(dst, dst, esem.at[q]).wait()
            return carry

        lax.fori_loop(0, PER, one, 0)
        wide.begin(p)
        wide.own(p, widen)

    def activate(p):
        wide.last(p, widen)
        rows = prows(p)
        mean = jnp.sum(ssum[rows, :], axis=1, keepdims=True) / (TP * COLS)
        scale = lax.rsqrt(mean + EPS)
        gate = xacc[rows, 0:CH] * scale
        up = xacc[rows, CH : 2 * CH] * scale
        hbuf[t, rows, :] = (gate * jax.nn.sigmoid(gate) * up).astype(BF16)
        deep.begin(p)
        deep.own(p, lower)

    def leave(p):
        deep.last(p, lower)
        rows = slice(p * PROWS, (p + 1) * PROWS)
        obuf[rows, :] = hacc[rows, :].astype(BF16)
        for q in far_first(p):
            dz, dx = offsets(q)
            d = ((z + NZ - dz) % NZ) * NX + (x + NX - dx) % NX
            if q == 0:
                pltpu.make_async_copy(block(obuf, q), block(ret, s), osem.at[s]).start()
            else:
                rdma(block(obuf, q), block(ret, s), osem.at[SP], osem.at[s], (d, t)).start()

    def wave(j, carry):
        p = j % PIECES
        stage = j // PIECES - p * DELAY[0] // DELAY[1]

        @pl.when((p == 0) & (j < PIECES * PIECES))
        def _():
            enter(j // PIECES)

        @pl.when((stage >= 1) & (stage <= 4))
        def _():
            wide.arrivals(stage, p, widen)

        @pl.when(stage == 5)
        def _():
            activate(p)

        @pl.when((stage >= 6) & (stage <= 9))
        def _():
            deep.arrivals(stage - 5, p, lower)

        for piece in range(PIECES):

            @pl.when((stage == 10) & (p == piece))
            def _(piece=piece):
                leave(piece)

        return carry

    lax.fori_loop(0, PIECES * (11 + (PIECES - 1) * DELAY[0] // DELAY[1]), wave, 0)

    def arrive(d, carry):
        pltpu.make_async_copy(block(ret, d), block(ret, d), osem.at[d]).wait()
        return carry

    lax.fori_loop(0, SP, arrive, 0)

    got0 = jnp.dot(pick0[...], ret[...], preferred_element_type=F32)
    got1 = jnp.dot(pick1[...], ret[...], preferred_element_type=F32)
    routed = got0 * mixw[:, 3:4] + got1 * mixw[:, 4:5]
    out[...] = resid[...].astype(F32) + routed

    for halo in halos:
        halo.wait_send()
    rest = bbuf.at[0:15]
    pltpu.make_async_copy(rest, rest, bss).wait()
    rest = send.at[0 : SLOTS - CAP]
    pltpu.make_async_copy(rest, rest, esem.at[SP]).wait()
    wide.drain()
    deep.drain()
    rest = obuf.at[0 : SLOTS - CAP]
    pltpu.make_async_copy(rest, rest, osem.at[SP]).wait()


def per_device(
    outer_gate, inner_gate, conv_input, conv_weight, doc_ids, output_weight, residual,
    norm_gain, expert_ids, group_weight, expert_weight, gate_weight, up_weight, down_weight,
):
    dma = pltpu.SemaphoreType.DMA
    vmem = pl.BlockSpec(memory_space=pltpu.VMEM)
    hbm = pl.BlockSpec(memory_space=pl.ANY)
    scratch = [
        pltpu.VMEM((TP * CH, COLS), BF16),
        pltpu.VMEM((TP * COLS, 2 * CH), BF16),
        pltpu.VMEM((TP * CH, COLS), BF16),
        dma((4,)),
        pltpu.VMEM((264, CH), F32),
        pltpu.VMEM((264, CH), F32),
        pltpu.VMEM((8, CH), F32),
        pltpu.VMEM((8, CH), F32),
        dma((4,)),
        pltpu.VMEM((TP, BROWS, CH), BF16),
        pltpu.VMEM((BROWS, COLS), F32),
        dma((NY, 3)),
        dma((NY, 3)),
        dma,
        pltpu.VMEM((ROWS, COLS), BF16),
        pltpu.VMEM((SLOTS, ROWS), BF16),
        pltpu.VMEM((ROWS, SLOTS), BF16),
        pltpu.VMEM((ROWS, SLOTS), BF16),
        pltpu.VMEM((ROWS, CH), F32),
        pltpu.VMEM((SLOTS, COLS), BF16),
        dma((SP + 1,)),
        pltpu.VMEM((TP, SLOTS, COLS), BF16),
        pltpu.VMEM((SLOTS, 2 * CH), F32),
        pltpu.VMEM((SLOTS, CH), F32),
        dma((NY, PIECES)),
        dma((NY, PIECES)),
        dma((2, PIECES)),
        dma,
        pltpu.VMEM((TP, SLOTS, CH), BF16),
        pltpu.VMEM((SLOTS, COLS), F32),
        dma((NY, PIECES)),
        dma((NY, PIECES)),
        dma((2, PIECES)),
        dma,
        pltpu.VMEM((SLOTS, COLS), BF16),
        pltpu.VMEM((SLOTS, COLS), BF16),
        dma((SP + 1,)),
    ]
    return pl.pallas_call(
        kernel,
        name="layer",
        out_shape=jax.ShapeDtypeStruct((ROWS, COLS), F32),
        in_specs=[vmem] * 10 + [hbm] * 4,
        out_specs=vmem,
        scratch_shapes=scratch,
        compiler_params=pltpu.CompilerParams(
            collective_id=0, has_side_effects=True, vmem_limit_bytes=56 * 1024 * 1024
        ),
    )(
        outer_gate,
        inner_gate,
        conv_input,
        conv_weight,
        doc_ids.reshape(1, ROWS),
        residual,
        norm_gain.reshape(2, CH),
        expert_ids.T,
        group_weight.reshape(1, ROWS),
        expert_weight.T,
        output_weight,
        gate_weight[0],
        up_weight[0],
        down_weight[0],
    ).astype(BF16)


def solution(mesh):
    return jax.shard_map(
        per_device,
        mesh=mesh,
        in_specs=(
            P("sp", "tp"),
            P("sp", "tp"),
            P("sp", "tp"),
            P(None, "tp"),
            P("sp"),
            P(None, "tp"),
            P("sp", "tp"),
            P("tp"),
            P("sp", None),
            P("sp"),
            P("sp", None),
            P("sp", None, "tp"),
            P("sp", None, "tp"),
            P("sp", None, "tp"),
        ),
        out_specs=P("sp", "tp"),
        check_vma=False,
    )
```
